128 devices in a mesh: sp: 16 (over z, y), tp: 8 (over x, core).
Axes of the slice: x: 4, y: 4, z: 4, core: 2. Of those that a mesh axis runs over, the one named last changes fastest.
Arguments:
- queries: bfloat16 [12288, 2048], P('sp', 'tp'), may hold values from -11 to 11
- key_rows: bfloat16 [12288, 2048], P('sp', 'tp'), may hold values from -4.5 to 4.5
- value_rows: bfloat16 [12288, 2048], P('sp', 'tp'), may hold values from -6 to 6
- log_forget: float32 [12288, 32], P('sp', 'tp'), may hold values from -1477.56 to 0, as said below
- stream_in: bfloat16 [12288, 2048], P('sp'), may hold values from -6 to 6
- out_weight: bfloat16 [2048, 2048], P('tp'), may hold values from -0.52734375 to 0.52734375
- mix_gain: float32 [2048], replicated, may hold values from 0.1 to 1.9
- mix_bias: float32 [2048], replicated, may hold values from -3 to 3
- gate_weight: bfloat16 [2048, 5632], P('sp', 'tp'), may hold values from -0.125 to 0.125
- up_weight: bfloat16 [2048, 5632], P('sp', 'tp'), may hold values from -0.125 to 0.125
- down_weight: bfloat16 [5632, 2048], P('tp', 'sp'), may hold values from -0.15917969 to 0.15917969
- ffn_gain: float32 [2048], replicated, may hold values from 0.1 to 1.9
- ffn_bias: float32 [2048], replicated, may hold values from -3 to 3
Outputs:
- layer_out: bfloat16 [12288, 2048], P(('sp', 'tp'))
The draws below stay inside these ranges and needn't reach their ends.
Inputs may be any that keep to these rules, and one draw needn't show every extreme that they name: `log_forget`: each column never rises along the positions.
All inputs are finite; a program needn't handle non-finite values.
Results may differ from the reference program's by a relative error of at most 0.015.
Values may be sent and summed in bfloat16 or wider, within the bound.
A program may use at most 128 MiB of HBM per device.

```python
import math
import jax
import jax.numpy as jnp
from jax import lax

D = 2048
HEAD_TOTAL = 32
FF = 5632
TOK_DEV = 768
SEQUENCE_LENGTH = 12288
N_SP = 16


def draw_queries(key, part):
    base_noise = jax.random.normal(jax.random.fold_in(key, 1), (SEQUENCE_LENGTH, D), jnp.float32)
    row_scale = jnp.exp(jax.random.uniform(jax.random.fold_in(key, 31), (SEQUENCE_LENGTH, 1), jnp.float32, -0.7, 1.6))
    base_noise = jnp.clip(base_noise * row_scale, -11.0, 11.0)
    return base_noise.astype(jnp.bfloat16)


def draw_key_rows(key, part):
    base_noise = jax.random.normal(jax.random.fold_in(key, 2), (SEQUENCE_LENGTH, D), jnp.float32)
    row_scale = jnp.exp(jax.random.uniform(jax.random.fold_in(key, 32), (SEQUENCE_LENGTH, 1), jnp.float32, -0.8, 0.8))
    base_noise = jnp.clip(base_noise * row_scale, -4.5, 4.5)
    return base_noise.astype(jnp.bfloat16)


def draw_log_forget(key, part):
    head_order = jax.random.permutation(jax.random.fold_in(key, 21), HEAD_TOTAL)
    sluggish_heads = head_order < HEAD_TOTAL // 2
    fast_rate = jnp.exp(jax.random.uniform(jax.random.fold_in(key, 22), (HEAD_TOTAL,), jnp.float32, math.log(1.0 / 100.0), math.log(1.0 / 30.0)))
    head_rate = jnp.where(sluggish_heads, 0.5 / SEQUENCE_LENGTH, fast_rate)
    block_count = SEQUENCE_LENGTH // TOK_DEV
    block_factor = jnp.exp(jax.random.uniform(jax.random.fold_in(key, 23), (block_count, HEAD_TOTAL), jnp.float32, math.log(0.5), math.log(2.0)))
    position_factor = jax.random.uniform(jax.random.fold_in(key, 24), (SEQUENCE_LENGTH, HEAD_TOTAL), jnp.float32, 0.25, 1.75)
    logarithm_increments = -head_rate[None, :] * jnp.repeat(block_factor, TOK_DEV, axis=0) * position_factor
    spike_locations = jax.random.randint(jax.random.fold_in(key, 25), (3, HEAD_TOTAL), 0, SEQUENCE_LENGTH)
    spike_lengths = jax.random.uniform(jax.random.fold_in(key, 26), (3, HEAD_TOTAL), jnp.float32, 0.22, 0.69)
    token_positions = jnp.arange(SEQUENCE_LENGTH, dtype=jnp.int32)
    for spike_index in range(3):
        spike_matches = (token_positions[:, None] == spike_locations[spike_index][None, :]) & sluggish_heads[None, :]
        logarithm_increments = logarithm_increments - jnp.where(spike_matches, spike_lengths[spike_index][None, :], 0.0)
    return jnp.cumsum(logarithm_increments, axis=0).astype(jnp.float32)


def levels(key, dims, cuts, low, largest):
    level, own = 1.0, jax.random.fold_in(key, 6)
    for axis_at, blocks in cuts:
        heights = jnp.exp(jax.random.uniform(jax.random.fold_in(own, axis_at), (blocks,), jnp.float32, low / len(cuts), largest / len(cuts)))
        level = level * jnp.repeat(heights, dims[axis_at] // blocks).reshape([-1 if axis == axis_at else 1 for axis in range(len(dims))])
    return level


def scatter_about(key, extent, width, most, split=(), kind=jnp.bfloat16):
    values = width * jax.random.normal(key, extent, jnp.float32)
    if split:
        values = values * levels(key, extent, split, -0.22, 0.18)
    return jnp.clip(values, -most, most).astype(kind)


def setup_inputs(seed: int = 0) -> dict:
    seeds = jax.random.split(jax.random.key(seed), 14)
    return {
        "queries": draw_queries(jax.random.fold_in(seeds[13], 71), 0),
        "key_rows": draw_key_rows(jax.random.fold_in(seeds[13], 71), 0),
        "value_rows": scatter_about(seeds[2], (SEQUENCE_LENGTH, D), 1.0, 6.0, ((0, 16), (1, 8))),
        "log_forget": draw_log_forget(jax.random.fold_in(seeds[13], 71), 0),
        "stream_in": scatter_about(seeds[4], (SEQUENCE_LENGTH, D), 1.0, 6.0, ((0, 16),)),
        "out_weight": scatter_about(seeds[5], (D, D), (4.0 * D ** -0.5), 0.52734375, ((0, 8),)),
        "mix_gain": jnp.clip(1.0 + 0.18 * jax.random.normal(seeds[6], (D,), jnp.float32), 0.1, 1.9),
        "mix_bias": scatter_about(seeds[7], (D,), 0.5, 3.0, (), jnp.float32),
        "gate_weight": scatter_about(seeds[8], (D, FF), D ** -0.5, 0.125, ((0, 16), (1, 8))),
        "up_weight": scatter_about(seeds[9], (D, FF), D ** -0.5, 0.125, ((0, 16), (1, 8))),
        "down_weight": scatter_about(seeds[10], (FF, D), (2.0 * FF ** -0.5), 0.15917969, ((0, 8), (1, 16))),
        "ffn_gain": jnp.clip(1.0 + 0.18 * jax.random.normal(seeds[11], (D,), jnp.float32), 0.1, 1.9),
        "ffn_bias": scatter_about(seeds[12], (D,), 0.5, 3.0, (), jnp.float32),
    }


ALPHA = 8.0 ** 0.25
EPSILON = 1e-05

def layer_norm(matrix, norm_gain, norm_shift):
    centred = matrix - lax.optimization_barrier(jnp.mean(matrix, axis=-1, keepdims=True))
    spread = lax.optimization_barrier(jnp.mean(centred * centred, axis=-1, keepdims=True))
    return centred * lax.rsqrt(spread + EPSILON) * norm_gain + norm_shift

def head_attention(query_head, key_head, value_head, gate_head):
    head_dim = query_head.shape[1]
    score_scale = head_dim ** (-0.5)
    key_pos = jnp.arange(SEQUENCE_LENGTH, dtype=jnp.int32)
    query_blocks = query_head.reshape(N_SP, TOK_DEV, head_dim)
    gate_blocks = gate_head.reshape(N_SP, TOK_DEV)

    def one_block(packed):
        query_block, gate_block, block_index = packed
        scores = jnp.dot(query_block, key_head.T, preferred_element_type=jnp.float32) * score_scale
        scores = scores + gate_block[:, None] - gate_head[None, :]
        query_pos = block_index * TOK_DEV + jnp.arange(TOK_DEV, dtype=jnp.int32)
        allowed = key_pos[None, :] <= query_pos[:, None]
        masked = jnp.where(allowed, scores, -1e+30)
        highest = lax.optimization_barrier(jnp.max(masked, axis=1, keepdims=True))
        exponent = jnp.where(allowed, jnp.exp(masked - highest), 0.0)
        totals = lax.optimization_barrier(jnp.sum(exponent, axis=1, keepdims=True))
        weighted = jnp.dot(exponent.astype(jnp.bfloat16), value_head, preferred_element_type=jnp.float32)
        return (weighted / totals).astype(jnp.bfloat16)
    return lax.map(one_block, (query_blocks, gate_blocks, jnp.arange(N_SP, dtype=jnp.int32)))

def reference(queries, key_rows, value_rows, log_forget, stream_in, out_weight, mix_gain, mix_bias, gate_weight, up_weight, down_weight, ffn_gain, ffn_bias):
    head_count = log_forget.shape[1]
    head_dim = queries.shape[1] // head_count

    def split_heads(matrix):
        return matrix.reshape(SEQUENCE_LENGTH, head_count, head_dim).transpose(1, 0, 2)

    def per_head(packed):
        return head_attention(packed[0], packed[1], packed[2], packed[3])
    attended = lax.map(per_head, (split_heads(queries), split_heads(key_rows), split_heads(value_rows), log_forget.T))
    attended = attended.reshape(head_count, SEQUENCE_LENGTH, head_dim).transpose(1, 0, 2).reshape(SEQUENCE_LENGTH, head_count * head_dim)
    mix_out = jnp.dot(attended, out_weight, preferred_element_type=jnp.float32).astype(jnp.bfloat16)
    mix_out = lax.optimization_barrier(mix_out).astype(jnp.float32)
    normed = layer_norm(ALPHA * stream_in.astype(jnp.float32) + mix_out, mix_gain, mix_bias).astype(jnp.bfloat16)
    gate_part = jnp.dot(normed, gate_weight, preferred_element_type=jnp.float32)
    up_part = jnp.dot(normed, up_weight, preferred_element_type=jnp.float32)
    hidden = (jax.nn.silu(gate_part) * up_part).astype(jnp.bfloat16)
    lowered = jnp.dot(hidden, down_weight, preferred_element_type=jnp.float32).astype(jnp.bfloat16)
    lowered = lax.optimization_barrier(lowered).astype(jnp.float32)
    result = layer_norm(ALPHA * normed.astype(jnp.float32) + lowered, ffn_gain, ffn_bias)
    return result.astype(jnp.bfloat16)
```

```python
import functools

import jax
import jax.numpy as jnp
from jax import lax
from jax.experimental import pallas as pl
from jax.experimental.pallas import tpu as pltpu
from jax.sharding import PartitionSpec as P

ALPHA = 8.0**0.25
EPSILON = 1e-05
MESH = pl.DeviceIdType.MESH
LOG2E = 1.4426950408889634
NEG = -1e30
BL = 768
QW = 512
NT = 6
NB = 16
HD = 64
KVR = 144
VMEM = pl.BlockSpec(memory_space=pltpu.VMEM)
ANY = pl.BlockSpec(memory_space=pl.ANY)


def layer_norm(matrix, norm_gain, norm_shift):
    centred = matrix - jnp.mean(matrix, axis=-1, keepdims=True)
    spread = jnp.mean(centred * centred, axis=-1, keepdims=True)
    return centred * lax.rsqrt(spread + EPSILON) * norm_gain + norm_shift


def parts(x):
    hi = x.astype(jnp.bfloat16).astype(jnp.float32)
    rest = x - hi
    mid = rest.astype(jnp.bfloat16).astype(jnp.float32)
    return hi, mid, rest - mid


def head_of(sp):
    z, y = sp // 4, sp % 4
    return (z // 2) * 2 + y // 2


def member_of(sp):
    z, y = sp // 4, sp % 4
    return (z % 2) * 2 + y % 2


def place_of(head, member):
    z = (head // 2) * 2 + member // 2
    y = (head % 2) * 2 + member % 2
    return z * 4 + y


def chunk_of(t, member):
    return (t // 2) * 8 + (member if t % 2 == 0 else 7 - member)


def exchange_kernel(q_ref, k_ref, v_ref, g_ref, kvl, qt, ksrc, qsrc, ks, kr, qs, qr):
    me = lax.axis_index("sp")
    z, y = me // 4, me % 4
    barrier = pltpu.get_barrier_semaphore()
    for o in range(1, 16):
        to = ((z + o // 4) % 4) * 4 + (y + o % 4) % 4
        pl.semaphore_signal(barrier, inc=1, device_id={"sp": to}, device_id_type=MESH)
    kt = k_ref[...].T
    vt = v_ref[...].T
    qtt = q_ref[...].T
    gates = g_ref[...]
    row = lax.broadcasted_iota(jnp.int32, (16, BL), 0)
    for h in range(4):
        g = gates[h : h + 1]
        first = jnp.broadcast_to(g[:, 0:1], (1, BL))
        rows = [jnp.ones((1, BL), jnp.float32)]
        rows += parts((first - g) * LOG2E) + parts(first * (-LOG2E))
        extra = jnp.zeros((16, BL), jnp.float32)
        for n, r in enumerate(rows):
            extra = jnp.where(row == n, r, extra)
        ksrc[h, 0:64] = kt[64 * h : 64 * h + 64]
        ksrc[h, 64:80] = extra.astype(jnp.bfloat16)
        ksrc[h, 80:144] = vt[64 * h : 64 * h + 64]
        for i in range(3):
            qsrc[3 * h + i] = qtt[64 * h : 64 * h + 64, 256 * i : 256 * i + 256]
    pl.semaphore_wait(barrier, 15)
    own = pltpu.make_async_copy(ksrc.at[head_of(me)], kvl.at[me], kr.at[me])
    own.start()
    sends = []
    for o in range(1, 16):
        to = ((z + o // 4) % 4) * 4 + (y + o % 4) % 4
        copy = pltpu.make_async_remote_copy(
            src_ref=ksrc.at[head_of(to)],
            dst_ref=kvl.at[me],
            send_sem=ks.at[o],
            recv_sem=kr.at[me],
            device_id={"sp": to},
            device_id_type=MESH,
        )
        copy.start()
        sends.append(copy)
    qsends = []
    for h in range(4):
        for i in range(3):
            n = 3 * h + i
            sub = 3 * me + i
            c, u = sub // 2, sub % 2
            r = c % 8
            high = r // 4
            member = r + high * (7 - 2 * r)
            slot = 2 * ((c // 8) * 2 + high) + u
            to = place_of(h, member)
            copy = pltpu.make_async_remote_copy(
                src_ref=qsrc.at[n],
                dst_ref=qt.at[slot],
                send_sem=qs.at[n],
                recv_sem=qr.at[slot],
                device_id={"sp": to},
                device_id_type=MESH,
            )
            local = pltpu.make_async_copy(qsrc.at[n], qt.at[slot], qr.at[slot])

            @pl.when(to != me)
            def _():
                copy.start()

            @pl.when(to == me)
            def _():
                local.start()

            qsends.append((to, copy))
    for copy in sends:
        copy.wait_send()
    for to, copy in qsends:

        @pl.when(to != me)
        def _():
            copy.wait_send()

    for b in range(NB):
        pltpu.make_async_copy(ksrc.at[0], kvl.at[b], kr.at[b]).wait()
    for s in range(2 * NT):
        pltpu.make_async_copy(qsrc.at[0], qt.at[s], qr.at[s]).wait()


def exchange(q, k, v, gates):
    return pl.pallas_call(
        exchange_kernel,
        name="exchange",
        out_shape=(
            jax.ShapeDtypeStruct((NB, KVR, BL), jnp.bfloat16),
            jax.ShapeDtypeStruct((2 * NT, HD, 256), jnp.bfloat16),
        ),
        in_specs=[VMEM] * 4,
        out_specs=(ANY, ANY),
        scratch_shapes=[
            pltpu.VMEM((4, KVR, BL), jnp.bfloat16),
            pltpu.VMEM((12, HD, 256), jnp.bfloat16),
            pltpu.SemaphoreType.DMA((16,)),
            pltpu.SemaphoreType.DMA((16,)),
            pltpu.SemaphoreType.DMA((12,)),
            pltpu.SemaphoreType.DMA((12,)),
        ],
        compiler_params=pltpu.CompilerParams(collective_id=0, has_side_effects=True),
        cost_estimate=pl.CostEstimate(flops=50 * 10**9, bytes_accessed=8 * 10**6, transcendentals=0),
    )(q, k, v, gates)


def attention_kernel(mm_ref, kvl, qt, o_ref, X, R, S0, S1, mx0, mx1, M, A, base):
    mm = mm_ref[0]
    for b in range(NB):
        X[b * BL : (b + 1) * BL, :] = kvl[b, 0:128, :].T
        gate_rows = kvl[b, 64:80, 0:128].astype(jnp.float32)
        base[b] = jnp.broadcast_to(gate_rows[4:5] + gate_rows[5:6] + gate_rows[6:7], (8, 128))
    row = lax.broadcasted_iota(jnp.int32, (64, QW), 0)
    ones = jnp.where((row >= 1) & (row < 4), 1.0, 0.0).astype(jnp.bfloat16)
    for t in range(NT):
        q = jnp.concatenate([qt[2 * t], qt[2 * t + 1]], axis=1).astype(jnp.float32)
        q = q * (LOG2E / 8)
        hi = q.astype(jnp.bfloat16)
        R[t, 0:64] = hi
        R[t, 64:128] = ones
        R[t, 128:192] = (q - hi.astype(jnp.float32)).astype(jnp.bfloat16)
        R[t, 192:256] = jnp.zeros((64, QW), jnp.bfloat16)
        M[t] = jnp.full((8, QW), NEG, jnp.float32)
        A[t] = jnp.zeros((80, QW), jnp.float32)

    def qk(b, t, S, mx):
        x = X[pl.ds(pl.multiple_of(b * BL, BL), BL), :]
        s = jnp.dot(
            jnp.concatenate([x, x], axis=1), R[t], preferred_element_type=jnp.float32
        )
        S[...] = s
        mx[...] = jnp.max(s.reshape(BL // 8, 8, QW), axis=0)

    def mask(b, c, S, mx):
        @pl.when(b * BL + BL > c * QW)
        def _():
            kp = b * BL + lax.broadcasted_iota(jnp.int32, (BL, QW), 0)
            qp = c * QW + lax.broadcasted_iota(jnp.int32, (BL, QW), 1)
            s = jnp.where(kp <= qp, S[...], NEG)
            S[...] = s
            mx[...] = jnp.max(s.reshape(BL // 8, 8, QW), axis=0)

    def pv(b, t, S, mx):
        m_old = M[t][0:1]
        bs = jnp.tile(base[b][0:1], (1, QW // 128))
        m_new = jnp.maximum(m_old, jnp.max(mx[...], axis=0, keepdims=True) + bs)
        p = jnp.exp2(S[...] - (m_new - bs)).astype(jnp.bfloat16)
        o = jnp.dot(kvl[b, 64:144], p, preferred_element_type=jnp.float32)
        A[t] = A[t] * jnp.exp2(m_old - m_new) + o
        M[t] = jnp.broadcast_to(m_new, (8, QW))

    for t in range(NT):
        c = chunk_of(t, mm)
        nb = lax.div(c * QW + QW - 1, BL) + 1
        qk(0, t, S0, mx0)
        mask(0, c, S0, mx0)

        def body(i, _):
            b = 2 * i
            nxt = jnp.minimum(b + 1, nb - 1)
            qk(nxt, t, S1, mx1)
            pv(b, t, S0, mx0)
            mask(nxt, c, S1, mx1)

            @pl.when(b + 1 < nb)
            def _():
                after = jnp.minimum(b + 2, nb - 1)
                qk(after, t, S0, mx0)
                pv(b + 1, t, S1, mx1)
                mask(after, c, S0, mx0)

            return 0

        lax.fori_loop(0, lax.div(nb + 1, 2), body, 0)
        a = A[t]
        o_ref[t] = (a[16:80] / a[0:1]).T.astype(jnp.bfloat16)


def attention(member, kvl, qt):
    return pl.pallas_call(
        attention_kernel,
        name="attention",
        out_shape=jax.ShapeDtypeStruct((NT, QW, HD), jnp.bfloat16),
        in_specs=[pl.BlockSpec(memory_space=pltpu.SMEM), VMEM, VMEM],
        out_specs=VMEM,
        scratch_shapes=[
            pltpu.VMEM((NB * BL, 128), jnp.bfloat16),
            pltpu.VMEM((NT, 256, QW), jnp.bfloat16),
            pltpu.VMEM((BL, QW), jnp.float32),
            pltpu.VMEM((BL, QW), jnp.float32),
            pltpu.VMEM((8, QW), jnp.float32),
            pltpu.VMEM((8, QW), jnp.float32),
            pltpu.VMEM((NT, 8, QW), jnp.float32),
            pltpu.VMEM((NT, 80, QW), jnp.float32),
            pltpu.VMEM((NB, 8, 128), jnp.float32),
        ],
        compiler_params=pltpu.CompilerParams(vmem_limit_bytes=48 * 2**20),
        cost_estimate=pl.CostEstimate(flops=40 * 10**9, bytes_accessed=8 * 10**6, transcendentals=0),
    )(member, kvl, qt)


def give_back_kernel(o_ref, att, ss, rs):
    me = lax.axis_index("sp")
    tp = lax.axis_index("tp")
    member = member_of(me)
    head = tp * 4 + head_of(me)
    for phase in range(2):
        for t in range(NT):
            c = chunk_of(t, member)
            for u in range(2):
                sub = 2 * c + u

                def one(w, _):
                    to_sp = sub // 3
                    piece = 8 * (sub % 3) + w
                    to_tp = piece // 3
                    spot = 32 * (piece % 3)
                    src = o_ref.at[t, pl.ds(pl.multiple_of(256 * u + 32 * w, 32), 32)]
                    dst = att.at[head, pl.ds(pl.multiple_of(spot, 32), 32)]
                    n = (2 * t + u) * 8 + w
                    copy = pltpu.make_async_remote_copy(
                        src_ref=src,
                        dst_ref=dst,
                        send_sem=ss.at[n],
                        recv_sem=rs,
                        device_id={"sp": to_sp, "tp": to_tp},
                        device_id_type=MESH,
                    )
                    mine = (to_sp == me) & (to_tp == tp)

                    @pl.when(jnp.logical_not(mine))
                    def _():
                        if phase == 0:
                            copy.start()
                        else:
                            copy.wait_send()

                    if phase == 0:

                        @pl.when(mine)
                        def _():
                            pltpu.make_async_copy(src, dst, rs).start()

                    return 0

                lax.fori_loop(0, 8, one, 0)
    pltpu.make_async_copy(att, att, rs).wait()


def give_back(o):
    return pl.pallas_call(
        give_back_kernel,
        name="give_back",
        out_shape=jax.ShapeDtypeStruct((32, 96, HD), jnp.bfloat16),
        in_specs=[VMEM],
        out_specs=ANY,
        scratch_shapes=[pltpu.SemaphoreType.DMA((96,)), pltpu.SemaphoreType.DMA],
        compiler_params=pltpu.CompilerParams(has_side_effects=True),
        cost_estimate=pl.CostEstimate(flops=10 * 10**9, bytes_accessed=10**6, transcendentals=0),
    )(o)


def body(
    queries,
    key_rows,
    value_rows,
    log_forget,
    stream_in,
    out_weight,
    mix_gain,
    mix_bias,
    gate_weight,
    up_weight,
    down_weight,
    ffn_gain,
    ffn_bias,
):
    member = member_of(lax.axis_index("sp")).astype(jnp.int32).reshape(1)
    kvl, qt = exchange(queries, key_rows, value_rows, log_forget.T)
    att = give_back(attention(member, kvl, qt))
    attended = att.transpose(1, 0, 2).reshape(96, 2048)
    offset = lax.axis_index("tp") * 96
    mixed = jnp.dot(
        attended,
        lax.all_gather(out_weight, "tp", axis=0, tiled=True),
        preferred_element_type=jnp.float32,
    )
    mix_out = lax.optimization_barrier(mixed.astype(jnp.bfloat16)).astype(jnp.float32)
    stream_own = lax.dynamic_slice_in_dim(stream_in, offset, 96, 0)
    normed = layer_norm(
        ALPHA * stream_own.astype(jnp.float32) + mix_out, mix_gain, mix_bias
    ).astype(jnp.bfloat16)
    gathered = lax.all_gather(normed, "tp", axis=0, tiled=True)
    both = lax.all_gather(
        jnp.concatenate([gate_weight, up_weight], axis=1), "sp", axis=0, tiled=True
    )
    gate_part = jnp.dot(gathered, both[:, :704], preferred_element_type=jnp.float32)
    up_part = jnp.dot(gathered, both[:, 704:], preferred_element_type=jnp.float32)
    hidden = (jax.nn.silu(gate_part) * up_part).astype(jnp.bfloat16)
    partial_terms = jnp.dot(
        hidden,
        lax.all_gather(down_weight, "sp", axis=1, tiled=True),
        preferred_element_type=jnp.float32,
    )
    lowered = lax.psum_scatter(
        partial_terms.astype(jnp.bfloat16), "tp", scatter_dimension=0, tiled=True
    ).astype(jnp.float32)
    lowered = lax.optimization_barrier(lowered.astype(jnp.bfloat16)).astype(jnp.float32)
    result = layer_norm(ALPHA * normed.astype(jnp.float32) + lowered, ffn_gain, ffn_bias)
    return result.astype(jnp.bfloat16)


def solution(mesh):
    placed = (
        P("sp", "tp"),
        P("sp", "tp"),
        P("sp", "tp"),
        P("sp", "tp"),
        P("sp", None),
        P("tp", None),
        P(),
        P(),
        P("sp", "tp"),
        P("sp", "tp"),
        P("tp", "sp"),
        P(),
        P(),
    )
    return jax.shard_map(
        body, mesh=mesh, in_specs=placed, out_specs=P(("sp", "tp"), None), check_vma=False
    )
```

```python
import functools

import jax
import jax.numpy as jnp
from jax import lax
from jax.experimental import pallas as pl
from jax.experimental.pallas import tpu as pltpu
from jax.sharding import PartitionSpec as P

ALPHA = 8.0**0.25
EPSILON = 1e-05
MESH = pl.DeviceIdType.MESH
LOG2E = 1.4426950408889634
NEG = -1e30
BL = 768
QW = 512
NT = 6
NB = 16
HD = 64
KVR = 144
VMEM = pl.BlockSpec(memory_space=pltpu.VMEM)
ANY = pl.BlockSpec(memory_space=pl.ANY)


def layer_norm(matrix, norm_gain, norm_shift):
    centred = matrix - jnp.mean(matrix, axis=-1, keepdims=True)
    spread = jnp.mean(centred * centred, axis=-1, keepdims=True)
    return centred * lax.rsqrt(spread + EPSILON) * norm_gain + norm_shift


def parts(x):
    hi = x.astype(jnp.bfloat16).astype(jnp.float32)
    rest = x - hi
    mid = rest.astype(jnp.bfloat16).astype(jnp.float32)
    return hi, mid, rest - mid


def head_of(sp):
    z, y = sp // 4, sp % 4
    return (z // 2) * 2 + y // 2


def member_of(sp):
    z, y = sp // 4, sp % 4
    return (z % 2) * 2 + y % 2


def place_of(head, member):
    z = (head // 2) * 2 + member // 2
    y = (head % 2) * 2 + member % 2
    return z * 4 + y


def chunk_of(t, member):
    return (t // 2) * 8 + (member if t % 2 == 0 else 7 - member)


def ring():
    tp = lax.axis_index("tp")
    x, core = tp // 2, tp % 2
    right = ((x + 1) % 4) * 2 + core
    left = ((x + 3) % 4) * 2 + core
    far = ((x + 2) % 4) * 2 + core
    return tp, x * 2 + 1 - core, right, left, far


def greet_ring():
    tp, sibling, right, left, far = ring()
    barrier = pltpu.get_barrier_semaphore()
    for peer in (sibling, right, left):
        pl.semaphore_signal(barrier, inc=1, device_id={"tp": peer}, device_id_type=MESH)


class RingGather:
    def __init__(self, own, buf, send, recv):
        self.own, self.buf, self.send, self.recv = own, buf, send, recv
        self.rows = buf.shape[1]
        self.half = self.rows // 2
        self.count = 0
        self.started = []

    def push(self, src, slot, peer, half=None):
        if half is None:
            dst, sem = self.buf.at[slot], self.recv.at[slot, 0]
        else:
            cut = pl.ds(half * self.half, self.half)
            dst, sem = self.buf.at[slot, cut], self.recv.at[slot, half]
        copy = pltpu.make_async_remote_copy(
            src_ref=src,
            dst_ref=dst,
            send_sem=self.send.at[self.count],
            recv_sem=sem,
            device_id={"tp": peer},
            device_id_type=MESH,
        )
        copy.start()
        self.count += 1
        self.started.append(copy)

    def part(self, slot, half):
        return self.buf.at[slot, pl.ds(half * self.half, self.half)]

    def arrive(self, slot, half=None):
        if half is None:
            ref, sem = self.buf.at[slot], self.recv.at[slot, 0]
        else:
            ref, sem = self.part(slot, half), self.recv.at[slot, half]
        pltpu.make_async_copy(ref, ref, sem).wait()

    def begin(self):
        tp, sibling, right, left, far = ring()
        self.push(self.own, tp, right)
        self.push(self.own, tp, left)
        self.push(self.own, tp, sibling)

    def relay(self):
        tp, sibling, right, left, far = ring()
        self.arrive(left)
        self.push(self.part(left, 0), left, right, 0)
        self.push(self.buf.at[left], left, sibling)
        self.arrive(right)
        self.push(self.part(right, 1), right, left, 1)
        self.push(self.buf.at[right], right, sibling)
        for half in range(2):
            self.arrive(far, half)
            self.push(self.part(far, half), far, sibling, half)

    def finish(self):
        tp, sibling, right, left, far = ring()
        x = tp // 2
        other = 1 - tp % 2
        self.arrive(sibling)
        self.arrive(((x + 3) % 4) * 2 + other)
        self.arrive(((x + 1) % 4) * 2 + other)
        for half in range(2):
            self.arrive(((x + 2) % 4) * 2 + other, half)
        for copy in self.started:
            copy.wait_send()


def exchange_kernel(
    q_ref, k_ref, v_ref, g_ref, w_ref, kvl, qt, wall, ksrc, qsrc, wsrc, ks, kr, qs, qr, ws, wr, wl
):
    me = lax.axis_index("sp")
    z, y = me // 4, me % 4
    barrier = pltpu.get_barrier_semaphore()
    for o in range(1, 16):
        to = ((z + o // 4) % 4) * 4 + (y + o % 4) % 4
        pl.semaphore_signal(barrier, inc=1, device_id={"sp": to}, device_id_type=MESH)
    greet_ring()
    tp = lax.axis_index("tp")
    load = pltpu.make_async_copy(w_ref, wsrc, wl.at[0])
    load.start()
    kt = k_ref[...].T
    vt = v_ref[...].T
    qtt = q_ref[...].T
    gates = g_ref[...]
    row = lax.broadcasted_iota(jnp.int32, (16, BL), 0)
    for h in range(4):
        g = gates[h : h + 1]
        first = jnp.broadcast_to(g[:, 0:1], (1, BL))
        rows = [jnp.ones((1, BL), jnp.float32)]
        rows += parts((first - g) * LOG2E) + parts(first * (-LOG2E))
        extra = jnp.zeros((16, BL), jnp.float32)
        for n, r in enumerate(rows):
            extra = jnp.where(row == n, r, extra)
        ksrc[h, 0:64] = kt[64 * h : 64 * h + 64]
        ksrc[h, 64:80] = extra.astype(jnp.bfloat16)
        ksrc[h, 80:144] = vt[64 * h : 64 * h + 64]
        for i in range(3):
            qsrc[3 * h + i] = qtt[64 * h : 64 * h + 64, 256 * i : 256 * i + 256]
    load.wait()
    pl.semaphore_wait(barrier, 18)
    own = pltpu.make_async_copy(ksrc.at[head_of(me)], kvl.at[me], kr.at[me])
    own.start()
    sends = []
    for o in range(1, 16):
        to = ((z + o // 4) % 4) * 4 + (y + o % 4) % 4
        copy = pltpu.make_async_remote_copy(
            src_ref=ksrc.at[head_of(to)],
            dst_ref=kvl.at[me],
            send_sem=ks.at[o],
            recv_sem=kr.at[me],
            device_id={"sp": to},
            device_id_type=MESH,
        )
        copy.start()
        sends.append(copy)
    qsends = []
    for h in range(4):
        for i in range(3):
            n = 3 * h + i
            sub = 3 * me + i
            c, u = sub // 2, sub % 2
            r = c % 8
            high = r // 4
            member = r + high * (7 - 2 * r)
            slot = 2 * ((c // 8) * 2 + high) + u
            to = place_of(h, member)
            copy = pltpu.make_async_remote_copy(
                src_ref=qsrc.at[n],
                dst_ref=qt.at[slot],
                send_sem=qs.at[n],
                recv_sem=qr.at[slot],
                device_id={"sp": to},
                device_id_type=MESH,
            )
            local = pltpu.make_async_copy(qsrc.at[n], qt.at[slot], qr.at[slot])

            @pl.when(to != me)
            def _():
                copy.start()

            @pl.when(to == me)
            def _():
                local.start()

            qsends.append((to, copy))
    keep = pltpu.make_async_copy(wsrc, wall.at[tp], wl.at[1])
    keep.start()
    gather = RingGather(wsrc, wall, ws, wr)
    gather.begin()
    gather.relay()
    gather.finish()
    keep.wait()
    for copy in sends:
        copy.wait_send()
    for to, copy in qsends:

        @pl.when(to != me)
        def _():
            copy.wait_send()

    for b in range(NB):
        pltpu.make_async_copy(ksrc.at[0], kvl.at[b], kr.at[b]).wait()
    for s in range(2 * NT):
        pltpu.make_async_copy(qsrc.at[0], qt.at[s], qr.at[s]).wait()


def exchange(q, k, v, gates, w):
    return pl.pallas_call(
        exchange_kernel,
        name="exchange",
        out_shape=(
            jax.ShapeDtypeStruct((NB, KVR, BL), jnp.bfloat16),
            jax.ShapeDtypeStruct((2 * NT, HD, 256), jnp.bfloat16),
            jax.ShapeDtypeStruct((8, 256, 2048), jnp.bfloat16),
        ),
        in_specs=[VMEM] * 4 + [ANY],
        out_specs=(ANY, ANY, ANY),
        scratch_shapes=[
            pltpu.VMEM((4, KVR, BL), jnp.bfloat16),
            pltpu.VMEM((12, HD, 256), jnp.bfloat16),
            pltpu.VMEM((256, 2048), jnp.bfloat16),
            pltpu.SemaphoreType.DMA((16,)),
            pltpu.SemaphoreType.DMA((16,)),
            pltpu.SemaphoreType.DMA((12,)),
            pltpu.SemaphoreType.DMA((12,)),
            pltpu.SemaphoreType.DMA((9,)),
            pltpu.SemaphoreType.DMA((8, 2)),
            pltpu.SemaphoreType.DMA((2,)),
        ],
        compiler_params=pltpu.CompilerParams(collective_id=0, has_side_effects=True),
        cost_estimate=pl.CostEstimate(flops=50 * 10**9, bytes_accessed=8 * 10**6, transcendentals=0),
    )(q, k, v, gates, w)


def attention_kernel(mm_ref, kvl, qt, o_ref, X, R, S0, S1, mx0, mx1, M, A, base):
    mm = mm_ref[0]
    for b in range(NB):
        X[b * BL : (b + 1) * BL, :] = kvl[b, 0:128, :].T
        gate_rows = kvl[b, 64:80, 0:128].astype(jnp.float32)
        base[b] = jnp.broadcast_to(gate_rows[4:5] + gate_rows[5:6] + gate_rows[6:7], (8, 128))
    row = lax.broadcasted_iota(jnp.int32, (64, QW), 0)
    ones = jnp.where((row >= 1) & (row < 4), 1.0, 0.0).astype(jnp.bfloat16)
    for t in range(NT):
        q = jnp.concatenate([qt[2 * t], qt[2 * t + 1]], axis=1).astype(jnp.float32)
        q = q * (LOG2E / 8)
        hi = q.astype(jnp.bfloat16)
        R[t, 0:64] = hi
        R[t, 64:128] = ones
        R[t, 128:192] = (q - hi.astype(jnp.float32)).astype(jnp.bfloat16)
        R[t, 192:256] = jnp.zeros((64, QW), jnp.bfloat16)
        M[t] = jnp.full((8, QW), NEG, jnp.float32)
        A[t] = jnp.zeros((80, QW), jnp.float32)

    def qk(b, t, S, mx):
        x = X[pl.ds(pl.multiple_of(b * BL, BL), BL), :]
        s = jnp.dot(
            jnp.concatenate([x, x], axis=1), R[t], preferred_element_type=jnp.float32
        )
        S[...] = s
        mx[...] = jnp.max(s.reshape(BL // 8, 8, QW), axis=0)

    def mask(b, c, S, mx):
        @pl.when(b * BL + BL > c * QW)
        def _():
            kp = b * BL + lax.broadcasted_iota(jnp.int32, (BL, QW), 0)
            qp = c * QW + lax.broadcasted_iota(jnp.int32, (BL, QW), 1)
            s = jnp.where(kp <= qp, S[...], NEG)
            S[...] = s
            mx[...] = jnp.max(s.reshape(BL // 8, 8, QW), axis=0)

    def pv(b, t, S, mx):
        m_old = M[t][0:1]
        bs = jnp.tile(base[b][0:1], (1, QW // 128))
        m_new = jnp.maximum(m_old, jnp.max(mx[...], axis=0, keepdims=True) + bs)
        p = jnp.exp2(S[...] - (m_new - bs)).astype(jnp.bfloat16)
        o = jnp.dot(kvl[b, 64:144], p, preferred_element_type=jnp.float32)
        A[t] = A[t] * jnp.exp2(m_old - m_new) + o
        M[t] = jnp.broadcast_to(m_new, (8, QW))

    for t in range(NT):
        c = chunk_of(t, mm)
        nb = lax.div(c * QW + QW - 1, BL) + 1
        qk(0, t, S0, mx0)
        mask(0, c, S0, mx0)

        def body(i, _):
            b = 2 * i
            nxt = jnp.minimum(b + 1, nb - 1)
            qk(nxt, t, S1, mx1)
            pv(b, t, S0, mx0)
            mask(nxt, c, S1, mx1)

            @pl.when(b + 1 < nb)
            def _():
                after = jnp.minimum(b + 2, nb - 1)
                qk(after, t, S0, mx0)
                pv(b + 1, t, S1, mx1)
                mask(after, c, S0, mx0)

            return 0

        lax.fori_loop(0, lax.div(nb + 1, 2), body, 0)
        a = A[t]
        o_ref[t] = (a[16:80] / a[0:1]).T.astype(jnp.bfloat16)


def attention(member, kvl, qt):
    return pl.pallas_call(
        attention_kernel,
        name="attention",
        out_shape=jax.ShapeDtypeStruct((NT, QW, HD), jnp.bfloat16),
        in_specs=[pl.BlockSpec(memory_space=pltpu.SMEM), VMEM, VMEM],
        out_specs=VMEM,
        scratch_shapes=[
            pltpu.VMEM((NB * BL, 128), jnp.bfloat16),
            pltpu.VMEM((NT, 256, QW), jnp.bfloat16),
            pltpu.VMEM((BL, QW), jnp.float32),
            pltpu.VMEM((BL, QW), jnp.float32),
            pltpu.VMEM((8, QW), jnp.float32),
            pltpu.VMEM((8, QW), jnp.float32),
            pltpu.VMEM((NT, 8, QW), jnp.float32),
            pltpu.VMEM((NT, 80, QW), jnp.float32),
            pltpu.VMEM((NB, 8, 128), jnp.float32),
        ],
        compiler_params=pltpu.CompilerParams(vmem_limit_bytes=48 * 2**20),
        cost_estimate=pl.CostEstimate(flops=40 * 10**9, bytes_accessed=8 * 10**6, transcendentals=0),
    )(member, kvl, qt)


def give_back_kernel(o_ref, att, ss, rs):
    me = lax.axis_index("sp")
    tp = lax.axis_index("tp")
    member = member_of(me)
    head = tp * 4 + head_of(me)
    for phase in range(2):
        for t in range(NT):
            c = chunk_of(t, member)
            for u in range(2):
                sub = 2 * c + u

                def one(w, _):
                    to_sp = sub // 3
                    piece = 8 * (sub % 3) + w
                    to_tp = piece // 3
                    spot = 32 * (piece % 3)
                    src = o_ref.at[t, pl.ds(pl.multiple_of(256 * u + 32 * w, 32), 32)]
                    dst = att.at[head, pl.ds(pl.multiple_of(spot, 32), 32)]
                    n = (2 * t + u) * 8 + w
                    copy = pltpu.make_async_remote_copy(
                        src_ref=src,
                        dst_ref=dst,
                        send_sem=ss.at[n],
                        recv_sem=rs,
                        device_id={"sp": to_sp, "tp": to_tp},
                        device_id_type=MESH,
                    )
                    mine = (to_sp == me) & (to_tp == tp)

                    @pl.when(jnp.logical_not(mine))
                    def _():
                        if phase == 0:
                            copy.start()
                        else:
                            copy.wait_send()

                    if phase == 0:

                        @pl.when(mine)
                        def _():
                            pltpu.make_async_copy(src, dst, rs).start()

                    return 0

                lax.fori_loop(0, 8, one, 0)
    pltpu.make_async_copy(att, att, rs).wait()


def give_back(o):
    return pl.pallas_call(
        give_back_kernel,
        name="give_back",
        out_shape=jax.ShapeDtypeStruct((32, 96, HD), jnp.bfloat16),
        in_specs=[VMEM],
        out_specs=ANY,
        scratch_shapes=[pltpu.SemaphoreType.DMA((96,)), pltpu.SemaphoreType.DMA],
        compiler_params=pltpu.CompilerParams(has_side_effects=True),
        cost_estimate=pl.CostEstimate(flops=10 * 10**9, bytes_accessed=10**6, transcendentals=0),
    )(o)


def mix_kernel(att, w_ref, stream, gain, bias, out, lhs, wbuf, res, ws, rs, send, recv):
    tp = lax.axis_index("tp")
    greet_ring()
    loads = [pltpu.make_async_copy(w_ref.at[j], wbuf.at[j], ws.at[j]) for j in range(8)]
    for load in loads:
        load.start()
    own = pltpu.make_async_copy(
        stream.at[pl.ds(pl.multiple_of(tp * 96, 96), 96)], res, rs
    )
    own.start()
    for h in range(32):
        lhs[:, HD * h : HD * h + HD] = att[h]
    total = None
    for j in range(8):
        loads[j].wait()
        term = jnp.dot(
            lhs[:, 256 * j : 256 * j + 256], wbuf[j], preferred_element_type=jnp.float32
        )
        total = term if total is None else total + term
    own.wait()
    mixed = total.astype(jnp.bfloat16).astype(jnp.float32)
    p = ALPHA * res[...].astype(jnp.float32) + mixed
    out[tp] = layer_norm(p, gain[...], bias[...]).astype(jnp.bfloat16)
    pl.semaphore_wait(pltpu.get_barrier_semaphore(), 3)
    gather = RingGather(out.at[tp], out, send, recv)
    gather.begin()
    gather.relay()
    gather.finish()


def mix(att, w, stream, gain, bias):
    return pl.pallas_call(
        mix_kernel,
        name="mix",
        out_shape=jax.ShapeDtypeStruct((8, 96, 2048), jnp.bfloat16),
        in_specs=[VMEM, ANY, ANY, VMEM, VMEM],
        out_specs=VMEM,
        scratch_shapes=[
            pltpu.VMEM((96, 2048), jnp.bfloat16),
            pltpu.VMEM((8, 256, 2048), jnp.bfloat16),
            pltpu.VMEM((96, 2048), jnp.bfloat16),
            pltpu.SemaphoreType.DMA((8,)),
            pltpu.SemaphoreType.DMA,
            pltpu.SemaphoreType.DMA((9,)),
            pltpu.SemaphoreType.DMA((8, 2)),
        ],
        compiler_params=pltpu.CompilerParams(collective_id=1, has_side_effects=True),
        cost_estimate=pl.CostEstimate(flops=20 * 10**9, bytes_accessed=10**7, transcendentals=0),
    )(att, w, stream, gain, bias)


def ffn_kernel(
    rows, both, down, gain, bias, out, wgu, wd, hid, pb, sib, z, rel, inn, wl, ss, sr, zs, zr
):
    tp = lax.axis_index("tp")
    x, core = tp // 2, tp % 2
    _, sibling, right, left, far = ring()
    greet_ring()
    load_gu = pltpu.make_async_copy(both, wgu, wl.at[0])
    load_gu.start()
    load_d = pltpu.make_async_copy(down, wd, wl.at[1])
    load_d.start()
    load_gu.wait()

    def up(i, _):
        r = rows[pl.ds(pl.multiple_of(i * 384, 384), 384), :]
        gate = jnp.dot(r, wgu[:, :704], preferred_element_type=jnp.float32)
        upper = jnp.dot(r, wgu[:, 704:], preferred_element_type=jnp.float32)
        hid[pl.ds(pl.multiple_of(i * 384, 384), 384), :] = (
            gate / (1.0 + jnp.exp(-gate)) * upper
        ).astype(jnp.bfloat16)
        return 0

    lax.fori_loop(0, 2, up, 0)
    load_d.wait()
    pl.semaphore_wait(pltpu.get_barrier_semaphore(), 3)
    chips = [(x + 2) % 4, (x + 1) % 4, (x + 3) % 4, x]

    def to_sibling(n):
        return pltpu.make_async_remote_copy(
            src_ref=pb.at[n, 1 - core],
            dst_ref=sib.at[n],
            send_sem=ss.at[n],
            recv_sem=sr.at[n],
            device_id={"tp": sibling},
            device_id_type=MESH,
        )

    def send(n, src, dst, peer):
        return pltpu.make_async_remote_copy(
            src_ref=src,
            dst_ref=dst,
            send_sem=zs.at[n],
            recv_sem=zr.at[n],
            device_id={"tp": peer},
            device_id_type=MESH,
        )

    hops = [
        send(0, z.at[0, pl.ds(0, 48)], rel.at[0], right),
        send(1, z.at[0, pl.ds(48, 48)], rel.at[1], left),
        send(2, z.at[1], inn.at[0], right),
        send(3, z.at[2], inn.at[1], left),
    ]

    def product(n):
        h = hid[pl.ds(pl.multiple_of(chips[n] * 192, 192), 192), :]
        s = jnp.dot(h, wd[...], preferred_element_type=jnp.float32).astype(jnp.bfloat16)
        pb[n, 0] = s[:96]
        pb[n, 1] = s[96:]
        to_sibling(n).start()

    def pair(n):
        to_sibling(n).wait_recv()
        return pb[n, core].astype(jnp.float32) + sib[n].astype(jnp.float32)

    product(0)
    product(1)
    z[0] = pair(0).astype(jnp.bfloat16)
    hops[0].start()
    hops[1].start()
    product(2)
    s = pair(1)
    hops[0].wait_recv()
    z[1, 0:48] = (s[:48] + rel[0].astype(jnp.float32)).astype(jnp.bfloat16)
    z[1, 48:96] = s[48:].astype(jnp.bfloat16)
    hops[2].start()
    product(3)
    s = pair(2)
    hops[1].wait_recv()
    z[2, 0:48] = s[:48].astype(jnp.bfloat16)
    z[2, 48:96] = (s[48:] + rel[1].astype(jnp.float32)).astype(jnp.bfloat16)
    hops[3].start()
    s = pair(3)
    hops[2].wait_recv()
    hops[3].wait_recv()
    s = s + inn[0].astype(jnp.float32) + inn[1].astype(jnp.float32)
    lowered = s.astype(jnp.bfloat16).astype(jnp.float32)
    normed = rows[pl.ds(pl.multiple_of(tp * 96, 96), 96), :].astype(jnp.float32)
    out[...] = layer_norm(ALPHA * normed + lowered, gain[...], bias[...]).astype(jnp.bfloat16)
    for n in range(4):
        to_sibling(n).wait_send()
        hops[n].wait_send()


def ffn(rows, both, down, gain, bias):
    return pl.pallas_call(
        ffn_kernel,
        name="ffn",
        out_shape=jax.ShapeDtypeStruct((96, 2048), jnp.bfloat16),
        in_specs=[VMEM, ANY, ANY, VMEM, VMEM],
        out_specs=VMEM,
        scratch_shapes=[
            pltpu.VMEM((2048, 1408), jnp.bfloat16),
            pltpu.VMEM((704, 2048), jnp.bfloat16),
            pltpu.VMEM((768, 704), jnp.bfloat16),
            pltpu.VMEM((4, 2, 96, 2048), jnp.bfloat16),
            pltpu.VMEM((4, 96, 2048), jnp.bfloat16),
            pltpu.VMEM((3, 96, 2048), jnp.bfloat16),
            pltpu.VMEM((2, 48, 2048), jnp.bfloat16),
            pltpu.VMEM((2, 96, 2048), jnp.bfloat16),
            pltpu.SemaphoreType.DMA((2,)),
            pltpu.SemaphoreType.DMA((4,)),
            pltpu.SemaphoreType.DMA((4,)),
            pltpu.SemaphoreType.DMA((4,)),
            pltpu.SemaphoreType.DMA((4,)),
        ],
        compiler_params=pltpu.CompilerParams(collective_id=2, has_side_effects=True),
        cost_estimate=pl.CostEstimate(flops=20 * 10**9, bytes_accessed=10**7, transcendentals=0),
    )(rows, both, down, gain, bias)


def body(
    queries,
    key_rows,
    value_rows,
    log_forget,
    stream_in,
    out_weight,
    mix_gain,
    mix_bias,
    gate_weight,
    up_weight,
    down_weight,
    ffn_gain,
    ffn_bias,
):
    member = member_of(lax.axis_index("sp")).astype(jnp.int32).reshape(1)
    kvl, qt, wall = exchange(queries, key_rows, value_rows, log_forget.T, out_weight)
    att = give_back(attention(member, kvl, qt))
    normed = mix(att, wall, stream_in, mix_gain[None], mix_bias[None])
    both = lax.all_gather(
        jnp.concatenate([gate_weight, up_weight], axis=1), "sp", axis=0, tiled=True
    )
    down = lax.all_gather(down_weight, "sp", axis=1, tiled=True)
    return ffn(normed.reshape(768, 2048), both, down, ffn_gain[None], ffn_bias[None])


def solution(mesh):
    placed = (
        P("sp", "tp"),
        P("sp", "tp"),
        P("sp", "tp"),
        P("sp", "tp"),
        P("sp", None),
        P("tp", None),
        P(),
        P(),
        P("sp", "tp"),
        P("sp", "tp"),
        P("tp", "sp"),
        P(),
        P(),
    )
    return jax.shard_map(
        body, mesh=mesh, in_specs=placed, out_specs=P(("sp", "tp"), None), check_vma=False
    )
```

```python
import functools

import jax
import jax.numpy as jnp
from jax import lax
from jax.experimental import pallas as pl
from jax.experimental.pallas import tpu as pltpu
from jax.sharding import PartitionSpec as P

ALPHA = 8.0**0.25
EPSILON = 1e-05
MESH = pl.DeviceIdType.MESH
LOG2E = 1.4426950408889634
NEG = -1e30
BL = 768
ORDER = tuple(range(1, 16))
RELAY = (8, 9, 14)
QW = 512
NT = 6
NB = 16
HD = 64
KVR = 144
VMEM = pl.BlockSpec(memory_space=pltpu.VMEM)
ANY = pl.BlockSpec(memory_space=pl.ANY)


def layer_norm(matrix, norm_gain, norm_shift):
    centred = matrix - jnp.mean(matrix, axis=-1, keepdims=True)
    spread = jnp.mean(centred * centred, axis=-1, keepdims=True)
    return centred * lax.rsqrt(spread + EPSILON) * norm_gain + norm_shift


def parts(x):
    hi = x.astype(jnp.bfloat16).astype(jnp.float32)
    rest = x - hi
    mid = rest.astype(jnp.bfloat16).astype(jnp.float32)
    return hi, mid, rest - mid


def head_of(sp):
    z, y = sp // 4, sp % 4
    return (z // 2) * 2 + y // 2


def member_of(sp):
    z, y = sp // 4, sp % 4
    return (z % 2) * 2 + y % 2


def place_of(head, member):
    z = (head // 2) * 2 + member // 2
    y = (head % 2) * 2 + member % 2
    return z * 4 + y


def chunk_of(t, member):
    return (t // 2) * 8 + (member if t % 2 == 0 else 7 - member)


def ring():
    tp = lax.axis_index("tp")
    x, core = tp // 2, tp % 2
    right = ((x + 1) % 4) * 2 + core
    left = ((x + 3) % 4) * 2 + core
    far = ((x + 2) % 4) * 2 + core
    return tp, x * 2 + 1 - core, right, left, far


def greet_ring():
    tp, sibling, right, left, far = ring()
    barrier = pltpu.get_barrier_semaphore()
    for peer in (sibling, right, left):
        pl.semaphore_signal(barrier, inc=1, device_id={"tp": peer}, device_id_type=MESH)


class RingGather:
    def __init__(self, own, buf, send, recv):
        self.own, self.buf, self.send, self.recv = own, buf, send, recv
        self.rows = buf.shape[1]
        self.half = self.rows // 2
        self.count = 0

    def push(self, src, slot, peer, half=None):
        if half is None:
            dst, sem = self.buf.at[slot], self.recv.at[slot, 0]
        else:
            cut = pl.ds(half * self.half, self.half)
            dst, sem = self.buf.at[slot, cut], self.recv.at[slot, half]
        copy = pltpu.make_async_remote_copy(
            src_ref=src,
            dst_ref=dst,
            send_sem=self.send.at[self.count],
            recv_sem=sem,
            device_id={"tp": peer},
            device_id_type=MESH,
        )
        copy.start()
        self.count += 1

    def part(self, slot, half):
        return self.buf.at[slot, pl.ds(half * self.half, self.half)]

    def arrive(self, slot, half=None):
        if half is None:
            ref, sem = self.buf.at[slot], self.recv.at[slot, 0]
        else:
            ref, sem = self.part(slot, half), self.recv.at[slot, half]
        pltpu.make_async_copy(ref, ref, sem).wait()

    def begin(self):
        tp, sibling, right, left, far = ring()
        self.count = 0
        self.push(self.own, tp, right)
        self.push(self.own, tp, left)
        self.push(self.own, tp, sibling)

    def stage(self, n):
        tp, sibling, right, left, far = ring()
        self.count = 3 + 2 * n
        if n == 0:
            self.arrive(left)
            self.push(self.part(left, 0), left, right, 0)
            self.push(self.buf.at[left], left, sibling)
        elif n == 1:
            self.arrive(right)
            self.push(self.part(right, 1), right, left, 1)
            self.push(self.buf.at[right], right, sibling)
        else:
            for half in range(2):
                self.arrive(far, half)
                self.push(self.part(far, half), far, sibling, half)

    def relay(self):
        for n in range(3):
            self.stage(n)

    def finish(self):
        tp, sibling, right, left, far = ring()
        x = tp // 2
        other = 1 - tp % 2
        self.arrive(sibling)
        self.arrive(((x + 3) % 4) * 2 + other)
        self.arrive(((x + 1) % 4) * 2 + other)
        for half in range(2):
            self.arrive(((x + 2) % 4) * 2 + other, half)
        for n in range(9):
            ref = self.own if n not in (3, 5, 7, 8) else self.part(0, 0)
            pltpu.make_async_copy(ref, ref, self.send.at[n]).wait()


def greet_all():
    me = lax.axis_index("sp")
    tp = lax.axis_index("tp")
    barrier = pltpu.get_barrier_semaphore()

    def one(i, _):
        sp = (me + i // 8) % 16
        to = (tp + i % 8) % 8
        pl.semaphore_signal(
            barrier, inc=1, device_id={"sp": sp, "tp": to}, device_id_type=MESH
        )
        return 0

    lax.fori_loop(1, 128, one, 0)


def attend_kernel(
    q_ref, k_ref, v_ref, g_ref, w_ref, att, wall,
    kvl, qt, ksrc, qsrc, wsrc, X, R, S0, S1, mx0, mx1, M, A, O,
    ks, kr, qs, qr, ws, wr, wl, gs, gr,
):
    me = lax.axis_index("sp")
    tp = lax.axis_index("tp")
    z, y = me // 4, me % 4
    greet_all()
    load = pltpu.make_async_copy(w_ref, wsrc, wl.at[0])
    load.start()
    kt = k_ref[...].T
    vt = v_ref[...].T
    qtt = q_ref[...].T
    gates = g_ref[...]
    row = lax.broadcasted_iota(jnp.int32, (16, BL), 0)
    for h in range(4):
        g = gates[h : h + 1]
        first = jnp.broadcast_to(g[:, 0:1], (1, BL))
        rows = [jnp.ones((1, BL), jnp.float32)]
        rows += parts((first - g) * LOG2E) + parts(first * (-LOG2E))
        extra = jnp.zeros((16, BL), jnp.float32)
        for n, r in enumerate(rows):
            extra = jnp.where(row == n, r, extra)
        ksrc[h, 0:64] = kt[64 * h : 64 * h + 64]
        ksrc[h, 64:80] = extra.astype(jnp.bfloat16)
        ksrc[h, 80:144] = vt[64 * h : 64 * h + 64]
        for i in range(3):
            qsrc[3 * h + i] = qtt[64 * h : 64 * h + 64, 256 * i : 256 * i + 256]
    load.wait()
    pl.semaphore_wait(pltpu.get_barrier_semaphore(), 127)
    qsends = []
    for h in range(4):
        for i in range(3):
            n = 3 * h + i
            sub = 3 * me + i
            c, u = sub // 2, sub % 2
            r = c % 8
            high = r // 4
            member = r + high * (7 - 2 * r)
            slot = 2 * ((c // 8) * 2 + high) + u
            to = place_of(h, member)
            copy = pltpu.make_async_remote_copy(
                src_ref=qsrc.at[n],
                dst_ref=qt.at[slot],
                send_sem=qs.at[n],
                recv_sem=qr.at[slot],
                device_id={"sp": to},
                device_id_type=MESH,
            )
            local = pltpu.make_async_copy(qsrc.at[n], qt.at[slot], qr.at[slot])

            @pl.when(to != me)
            def _():
                copy.start()

            @pl.when(to == me)
            def _():
                local.start()

            qsends.append((to, copy))
    sends = []
    for o in ORDER:
        to = ((z + o // 4) % 4) * 4 + (y + o % 4) % 4
        copy = pltpu.make_async_remote_copy(
            src_ref=ksrc.at[head_of(to)],
            dst_ref=kvl.at[me],
            send_sem=ks.at[o],
            recv_sem=kr.at[me],
            device_id={"sp": to},
            device_id_type=MESH,
        )
        copy.start()
        sends.append(copy)
    own = pltpu.make_async_copy(ksrc.at[head_of(me)], kvl.at[me], kr.at[me])
    own.start()
    keep = pltpu.make_async_copy(wsrc, wall.at[tp], wl.at[1])
    keep.start()
    gather = RingGather(wsrc, wall, ws, wr)
    gather.begin()

    row = lax.broadcasted_iota(jnp.int32, (64, QW), 0)
    ones = jnp.where((row >= 1) & (row < 4), 1.0, 0.0).astype(jnp.bfloat16)
    for t in range(NT):
        for u in range(2):
            pltpu.make_async_copy(qsrc.at[0], qt.at[2 * t + u], qr.at[2 * t + u]).wait()
        q = jnp.concatenate([qt[2 * t], qt[2 * t + 1]], axis=1).astype(jnp.float32)
        q = q * (LOG2E / 8)
        hi = q.astype(jnp.bfloat16)
        R[t, 0:64] = hi
        R[t, 64:128] = ones
        R[t, 128:192] = (q - hi.astype(jnp.float32)).astype(jnp.bfloat16)
        R[t, 192:256] = jnp.zeros((64, QW), jnp.bfloat16)
        M[t] = jnp.full((8, QW), NEG, jnp.float32)
        A[t] = jnp.zeros((80, QW), jnp.float32)

    mm = member_of(me)
    S = (S0, S1)
    mx = (mx0, mx1)

    def qk(t, n):
        x = X[...]
        s = jnp.dot(
            jnp.concatenate([x, x], axis=1), R[t], preferred_element_type=jnp.float32
        )
        S[n][...] = s
        mx[n][...] = jnp.max(s.reshape(BL // 8, 8, QW), axis=0)

    def mask(b, t, n):
        c = chunk_of(t, mm)

        @pl.when(b * BL + BL > c * QW)
        def _():
            kp = b * BL + lax.broadcasted_iota(jnp.int32, (BL, QW), 0)
            qp = c * QW + lax.broadcasted_iota(jnp.int32, (BL, QW), 1)
            s = jnp.where(kp <= qp, S[n][...], NEG)
            S[n][...] = s
            mx[n][...] = jnp.max(s.reshape(BL // 8, 8, QW), axis=0)

    def pv(b, t, n, bs):
        m_old = M[t][0:1]
        m_new = jnp.maximum(m_old, jnp.max(mx[n][...], axis=0, keepdims=True) + bs)
        p = jnp.exp2(S[n][...] - (m_new - bs)).astype(jnp.bfloat16)
        o = jnp.dot(kvl[b, 64:144], p, preferred_element_type=jnp.float32)
        A[t] = A[t] * jnp.exp2(m_old - m_new) + o
        M[t] = jnp.broadcast_to(m_new, (8, QW))

    def block(i, _):
        o = i
        b = ((z + 4 - o // 4) % 4) * 4 + (y + 4 - o % 4) % 4
        pltpu.make_async_copy(ksrc.at[0], kvl.at[b], kr.at[b]).wait()
        X[...] = kvl[b, 0:128, :].T
        g = kvl[b, 64:80, 0:128].astype(jnp.float32)
        bs = jnp.tile(g[4:5] + g[5:6] + g[6:7], (1, QW // 128))

        def live(t):
            return chunk_of(t, mm) * QW + QW > b * BL

        for t in range(NT):
            first = live(t) if t == 0 else live(t) & jnp.logical_not(live(t - 1))

            @pl.when(first)
            def _():
                qk(t, t % 2)
                mask(b, t, t % 2)

            @pl.when(live(t))
            def _():
                if t + 1 < NT:
                    qk(t + 1, (t + 1) % 2)
                pv(b, t, t % 2, bs)
                if t + 1 < NT:
                    mask(b, t + 1, (t + 1) % 2)

        for stage in range(3):

            @pl.when(i == RELAY[stage])
            def _():
                gather.stage(stage)

        return 0

    lax.fori_loop(0, 16, block, 0)

    head = tp * 4 + head_of(me)

    def piece(t, u, w):
        sub = 2 * chunk_of(t, mm) + u
        n = 8 * (sub % 3) + w
        to_sp, to_tp, spot = sub // 3, n // 3, n % 3
        src = O.at[(2 * t + u) * 8 + w]
        dst = att.at[head, spot]
        copy = pltpu.make_async_remote_copy(
            src_ref=src,
            dst_ref=dst,
            send_sem=gs.at[(2 * t + u) * 8 + w],
            recv_sem=gr,
            device_id={"sp": to_sp, "tp": to_tp},
            device_id_type=MESH,
        )
        return (to_sp == me) & (to_tp == tp), copy, src, dst

    for t in range(NT):
        a = A[t]
        out = (a[16:80] / a[0:1]).T.astype(jnp.bfloat16)
        for n in range(16):
            O[16 * t + n] = jnp.concatenate(
                [out[32 * n : 32 * n + 16], out[32 * n + 16 : 32 * n + 32]], axis=1
            )
    for t in range(NT):
        for u in range(2):

            def send(w, _):
                mine, copy, src, dst = piece(t, u, w)

                @pl.when(jnp.logical_not(mine))
                def _():
                    copy.start()

                @pl.when(mine)
                def _():
                    pltpu.make_async_copy(src, dst, gr).start()

                return 0

            lax.fori_loop(0, 8, send, 0)
    for t in range(NT):
        for u in range(2):

            def sent(w, _):
                mine, copy, src, dst = piece(t, u, w)

                @pl.when(jnp.logical_not(mine))
                def _():
                    copy.wait_send()

                return 0

            lax.fori_loop(0, 8, sent, 0)
    gather.finish()
    keep.wait()
    for copy in sends:
        copy.wait_send()
    for to, copy in qsends:

        @pl.when(to != me)
        def _():
            copy.wait_send()

    pltpu.make_async_copy(att, att, gr).wait()


def attend(q, k, v, gates, w):
    return pl.pallas_call(
        attend_kernel,
        name="attend",
        out_shape=(
            jax.ShapeDtypeStruct((32, 3, 16, 128), jnp.bfloat16),
            jax.ShapeDtypeStruct((8, 256, 2048), jnp.bfloat16),
        ),
        in_specs=[VMEM] * 4 + [ANY],
        out_specs=(ANY, ANY),
        scratch_shapes=[
            pltpu.VMEM((NB, KVR, BL), jnp.bfloat16),
            pltpu.VMEM((2 * NT, HD, 256), jnp.bfloat16),
            pltpu.VMEM((4, KVR, BL), jnp.bfloat16),
            pltpu.VMEM((12, HD, 256), jnp.bfloat16),
            pltpu.VMEM((256, 2048), jnp.bfloat16),
            pltpu.VMEM((BL, 128), jnp.bfloat16),
            pltpu.VMEM((NT, 256, QW), jnp.bfloat16),
            pltpu.VMEM((BL, QW), jnp.float32),
            pltpu.VMEM((BL, QW), jnp.float32),
            pltpu.VMEM((8, QW), jnp.float32),
            pltpu.VMEM((8, QW), jnp.float32),
            pltpu.VMEM((NT, 8, QW), jnp.float32),
            pltpu.VMEM((NT, 80, QW), jnp.float32),
            pltpu.VMEM((96, 16, 128), jnp.bfloat16),
            pltpu.SemaphoreType.DMA((16,)),
            pltpu.SemaphoreType.DMA((16,)),
            pltpu.SemaphoreType.DMA((12,)),
            pltpu.SemaphoreType.DMA((12,)),
            pltpu.SemaphoreType.DMA((9,)),
            pltpu.SemaphoreType.DMA((8, 2)),
            pltpu.SemaphoreType.DMA((2,)),
            pltpu.SemaphoreType.DMA((96,)),
            pltpu.SemaphoreType.DMA,
        ],
        compiler_params=pltpu.CompilerParams(
            collective_id=0, has_side_effects=True, vmem_limit_bytes=48 * 2**20
        ),
        cost_estimate=pl.CostEstimate(flops=90 * 10**9, bytes_accessed=8 * 10**6, transcendentals=0),
    )(q, k, v, gates, w)


class GridGather:
    def __init__(self, own, buf, send, recv):
        self.own, self.buf, self.send, self.recv = own, buf, send, recv
        self.half = buf.shape[0] // 2
        self.width = buf.shape[1] // 16

    def view(self, part, first, blocks=1):
        lanes = pl.ds(pl.multiple_of(first * self.width, self.width), blocks * self.width)
        return self.buf.at[pl.ds(part * self.half, self.half), lanes]

    def copy(self, n, src, dst, to):
        return pltpu.make_async_remote_copy(
            src_ref=src,
            dst_ref=dst,
            send_sem=self.send.at[n],
            recv_sem=self.recv.at[n],
            device_id={"sp": to},
            device_id_type=MESH,
        )

    def first(self):
        me = lax.axis_index("sp")
        z, y = me // 4, me % 4
        out = []
        for d in (1, 3, 2):
            to = (z * 4 + (y + d) % 4, ((z + d) % 4) * 4 + y)
            for part in range(2):
                src = self.own.at[pl.ds(part * self.half, self.half)]
                out.append(self.copy(2 * d + part, src, self.view(part, me), to[part]))
        return out

    def second(self):
        me = lax.axis_index("sp")
        z, y = me // 4, me % 4
        out = []
        for d in (1, 3, 2):
            strip = self.view(0, 4 * z, 4)
            out.append(self.copy(8 + d, strip, strip, ((z + d) % 4) * 4 + y))
            for k in range(4):
                one = self.view(1, 4 * k + y)
                out.append(self.copy(12 + 4 * (d - 1) + k, one, one, z * 4 + (y + d) % 4))
        return out


def mix_kernel(
    att, w_ref, stream, gain, bias, dw, out, wd, lhs, wbuf, res,
    ws, rs, send, recv, ds, dr,
):
    tp = lax.axis_index("tp")
    me = lax.axis_index("sp")
    z, y = me // 4, me % 4
    greet_ring()
    barrier = pltpu.get_barrier_semaphore()
    for d in (1, 2, 3):
        for to in (z * 4 + (y + d) % 4, ((z + d) % 4) * 4 + y):
            pl.semaphore_signal(barrier, inc=1, device_id={"sp": to}, device_id_type=MESH)
    loads = [pltpu.make_async_copy(w_ref.at[j], wbuf.at[j], ws.at[j]) for j in range(8)]
    for load in loads:
        load.start()
    own = pltpu.make_async_copy(
        stream.at[pl.ds(pl.multiple_of(tp * 96, 96), 96)], res, rs.at[0]
    )
    own.start()
    keep = pltpu.make_async_copy(
        dw, wd.at[:, pl.ds(pl.multiple_of(me * 128, 128), 128)], rs.at[1]
    )
    keep.start()
    pl.semaphore_wait(barrier, 9)
    down = GridGather(dw, wd, ds, dr)
    one = down.first()
    for copy in one:
        copy.start()
    for h in range(32):
        for n in range(3):
            lhs[32 * n : 32 * n + 16, HD * h : HD * h + HD] = att[h, n, :, 0:64]
            lhs[32 * n + 16 : 32 * n + 32, HD * h : HD * h + HD] = att[h, n, :, 64:128]
    total = None
    for j in range(8):
        loads[j].wait()
        term = jnp.dot(
            lhs[:, 256 * j : 256 * j + 256], wbuf[j], preferred_element_type=jnp.float32
        )
        total = term if total is None else total + term
    own.wait()
    mixed = total.astype(jnp.bfloat16).astype(jnp.float32)
    p = ALPHA * res[...].astype(jnp.float32) + mixed
    out[tp] = layer_norm(p, gain[...], bias[...]).astype(jnp.bfloat16)
    gather = RingGather(out.at[tp], out, send, recv)
    gather.begin()
    keep.wait()
    for copy in one:
        copy.wait_recv()
    two = down.second()
    for copy in two:
        copy.start()
    gather.relay()
    gather.finish()
    for copy in two:
        copy.wait_recv()
    for copy in one + two:
        copy.wait_send()


def mix(att, w, stream, gain, bias, dw):
    return pl.pallas_call(
        mix_kernel,
        name="mix",
        out_shape=(
            jax.ShapeDtypeStruct((8, 96, 2048), jnp.bfloat16),
            jax.ShapeDtypeStruct((704, 2048), jnp.bfloat16),
        ),
        in_specs=[VMEM, ANY, ANY, VMEM, VMEM, VMEM],
        out_specs=(VMEM, VMEM),
        scratch_shapes=[
            pltpu.VMEM((96, 2048), jnp.bfloat16),
            pltpu.VMEM((8, 256, 2048), jnp.bfloat16),
            pltpu.VMEM((96, 2048), jnp.bfloat16),
            pltpu.SemaphoreType.DMA((8,)),
            pltpu.SemaphoreType.DMA((2,)),
            pltpu.SemaphoreType.DMA((9,)),
            pltpu.SemaphoreType.DMA((8, 2)),
            pltpu.SemaphoreType.DMA((24,)),
            pltpu.SemaphoreType.DMA((24,)),
        ],
        compiler_params=pltpu.CompilerParams(collective_id=1, has_side_effects=True),
        cost_estimate=pl.CostEstimate(flops=20 * 10**9, bytes_accessed=10**7, transcendentals=0),
    )(att, w, stream, gain, bias, dw)


def ffn_kernel(
    rows, both, down, gain, bias, out, wgu, wd, hid, pb, sib, z, rel, inn, wl, ss, sr, zs, zr
):
    tp = lax.axis_index("tp")
    x, core = tp // 2, tp % 2
    _, sibling, right, left, far = ring()
    greet_ring()
    load_gu = pltpu.make_async_copy(both, wgu, wl.at[0])
    load_gu.start()
    load_d = pltpu.make_async_copy(down, wd, wl.at[1])
    load_d.start()
    load_gu.wait()

    def up(i, _):
        r = rows[pl.ds(pl.multiple_of(i * 384, 384), 384), :]
        gate = jnp.dot(r, wgu[:, :704], preferred_element_type=jnp.float32)
        upper = jnp.dot(r, wgu[:, 704:], preferred_element_type=jnp.float32)
        hid[pl.ds(pl.multiple_of(i * 384, 384), 384), :] = (
            gate / (1.0 + jnp.exp(-gate)) * upper
        ).astype(jnp.bfloat16)
        return 0

    lax.fori_loop(0, 2, up, 0)
    load_d.wait()
    pl.semaphore_wait(pltpu.get_barrier_semaphore(), 3)
    chips = [(x + 2) % 4, (x + 1) % 4, (x + 3) % 4, x]

    def to_sibling(n):
        return pltpu.make_async_remote_copy(
            src_ref=pb.at[n, 1 - core],
            dst_ref=sib.at[n],
            send_sem=ss.at[n],
            recv_sem=sr.at[n],
            device_id={"tp": sibling},
            device_id_type=MESH,
        )

    def send(n, src, dst, peer):
        return pltpu.make_async_remote_copy(
            src_ref=src,
            dst_ref=dst,
            send_sem=zs.at[n],
            recv_sem=zr.at[n],
            device_id={"tp": peer},
            device_id_type=MESH,
        )

    hops = [
        send(0, z.at[0, pl.ds(0, 48)], rel.at[0], right),
        send(1, z.at[0, pl.ds(48, 48)], rel.at[1], left),
        send(2, z.at[1], inn.at[0], right),
        send(3, z.at[2], inn.at[1], left),
    ]

    def product(n):
        h = hid[pl.ds(pl.multiple_of(chips[n] * 192, 192), 192), :]
        s = jnp.dot(h, wd[...], preferred_element_type=jnp.float32).astype(jnp.bfloat16)
        pb[n, 0] = s[:96]
        pb[n, 1] = s[96:]
        to_sibling(n).start()

    def pair(n):
        to_sibling(n).wait_recv()
        return pb[n, core].astype(jnp.float32) + sib[n].astype(jnp.float32)

    product(0)
    product(1)
    z[0] = pair(0).astype(jnp.bfloat16)
    hops[0].start()
    hops[1].start()
    product(2)
    s = pair(1)
    hops[0].wait_recv()
    z[1, 0:48] = (s[:48] + rel[0].astype(jnp.float32)).astype(jnp.bfloat16)
    z[1, 48:96] = s[48:].astype(jnp.bfloat16)
    hops[2].start()
    product(3)
    s = pair(2)
    hops[1].wait_recv()
    z[2, 0:48] = s[:48].astype(jnp.bfloat16)
    z[2, 48:96] = (s[48:] + rel[1].astype(jnp.float32)).astype(jnp.bfloat16)
    hops[3].start()
    s = pair(3)
    hops[2].wait_recv()
    hops[3].wait_recv()
    s = s + inn[0].astype(jnp.float32) + inn[1].astype(jnp.float32)
    lowered = s.astype(jnp.bfloat16).astype(jnp.float32)
    normed = rows[pl.ds(pl.multiple_of(tp * 96, 96), 96), :].astype(jnp.float32)
    out[...] = layer_norm(ALPHA * normed + lowered, gain[...], bias[...]).astype(jnp.bfloat16)
    for n in range(4):
        to_sibling(n).wait_send()
        hops[n].wait_send()


def ffn(rows, both, down, gain, bias):
    return pl.pallas_call(
        ffn_kernel,
        name="ffn",
        out_shape=jax.ShapeDtypeStruct((96, 2048), jnp.bfloat16),
        in_specs=[VMEM, ANY, ANY, VMEM, VMEM],
        out_specs=VMEM,
        scratch_shapes=[
            pltpu.VMEM((2048, 1408), jnp.bfloat16),
            pltpu.VMEM((704, 2048), jnp.bfloat16),
            pltpu.VMEM((768, 704), jnp.bfloat16),
            pltpu.VMEM((4, 2, 96, 2048), jnp.bfloat16),
            pltpu.VMEM((4, 96, 2048), jnp.bfloat16),
            pltpu.VMEM((3, 96, 2048), jnp.bfloat16),
            pltpu.VMEM((2, 48, 2048), jnp.bfloat16),
            pltpu.VMEM((2, 96, 2048), jnp.bfloat16),
            pltpu.SemaphoreType.DMA((2,)),
            pltpu.SemaphoreType.DMA((4,)),
            pltpu.SemaphoreType.DMA((4,)),
            pltpu.SemaphoreType.DMA((4,)),
            pltpu.SemaphoreType.DMA((4,)),
        ],
        compiler_params=pltpu.CompilerParams(collective_id=2, has_side_effects=True),
        cost_estimate=pl.CostEstimate(flops=20 * 10**9, bytes_accessed=10**7, transcendentals=0),
    )(rows, both, down, gain, bias)


def body(
    queries,
    key_rows,
    value_rows,
    log_forget,
    stream_in,
    out_weight,
    mix_gain,
    mix_bias,
    gate_weight,
    up_weight,
    down_weight,
    ffn_gain,
    ffn_bias,
):
    att, wall = attend(queries, key_rows, value_rows, log_forget.T, out_weight)
    normed, down = mix(att, wall, stream_in, mix_gain[None], mix_bias[None], down_weight)
    both = lax.all_gather(
        jnp.concatenate([gate_weight, up_weight], axis=1), "sp", axis=0, tiled=True
    )
    return ffn(normed.reshape(768, 2048), both, down, ffn_gain[None], ffn_bias[None])


def solution(mesh):
    placed = (
        P("sp", "tp"),
        P("sp", "tp"),
        P("sp", "tp"),
        P("sp", "tp"),
        P("sp", None),
        P("tp", None),
        P(),
        P(),
        P("sp", "tp"),
        P("sp", "tp"),
        P("tp", "sp"),
        P(),
        P(),
    )
    return jax.shard_map(
        body, mesh=mesh, in_specs=placed, out_specs=P(("sp", "tp"), None), check_vma=False
    )
```

```python
import functools

import jax
import jax.numpy as jnp
from jax import lax
from jax.experimental import pallas as pl
from jax.experimental.pallas import tpu as pltpu
from jax.sharding import PartitionSpec as P

ALPHA = 8.0**0.25
EPSILON = 1e-05
MESH = pl.DeviceIdType.MESH
LOG2E = 1.4426950408889634
NEG = -1e30
BL = 768
ORDER = tuple(range(1, 16))
RELAY = (8, 9, 14)
QW = 512
NT = 6
NB = 16
HD = 64
KVR = 144
VMEM = pl.BlockSpec(memory_space=pltpu.VMEM)
ANY = pl.BlockSpec(memory_space=pl.ANY)


def layer_norm(matrix, norm_gain, norm_shift):
    centred = matrix - jnp.mean(matrix, axis=-1, keepdims=True)
    spread = jnp.mean(centred * centred, axis=-1, keepdims=True)
    return centred * lax.rsqrt(spread + EPSILON) * norm_gain + norm_shift


def parts(x):
    hi = x.astype(jnp.bfloat16).astype(jnp.float32)
    rest = x - hi
    mid = rest.astype(jnp.bfloat16).astype(jnp.float32)
    return hi, mid, rest - mid


def head_of(sp):
    z, y = sp // 4, sp % 4
    return (z // 2) * 2 + y // 2


def member_of(sp):
    z, y = sp // 4, sp % 4
    return (z % 2) * 2 + y % 2


def place_of(head, member):
    z = (head // 2) * 2 + member // 2
    y = (head % 2) * 2 + member % 2
    return z * 4 + y


def chunk_of(t, member):
    return (t // 2) * 8 + (member if t % 2 == 0 else 7 - member)


def ring():
    tp = lax.axis_index("tp")
    x, core = tp // 2, tp % 2
    right = ((x + 1) % 4) * 2 + core
    left = ((x + 3) % 4) * 2 + core
    far = ((x + 2) % 4) * 2 + core
    return tp, x * 2 + 1 - core, right, left, far


def greet_ring():
    tp, sibling, right, left, far = ring()
    barrier = pltpu.get_barrier_semaphore()
    for peer in (sibling, right, left):
        pl.semaphore_signal(barrier, inc=1, device_id={"tp": peer}, device_id_type=MESH)


class RingGather:
    def __init__(self, own, buf, send, recv):
        self.own, self.buf, self.send, self.recv = own, buf, send, recv
        self.rows = buf.shape[1]
        self.half = self.rows // 2
        self.count = 0

    def push(self, src, slot, peer, half=None):
        if half is None:
            dst, sem = self.buf.at[slot], self.recv.at[slot, 0]
        else:
            cut = pl.ds(half * self.half, self.half)
            dst, sem = self.buf.at[slot, cut], self.recv.at[slot, half]
        copy = pltpu.make_async_remote_copy(
            src_ref=src,
            dst_ref=dst,
            send_sem=self.send.at[self.count],
            recv_sem=sem,
            device_id={"tp": peer},
            device_id_type=MESH,
        )
        copy.start()
        self.count += 1

    def part(self, slot, half):
        return self.buf.at[slot, pl.ds(half * self.half, self.half)]

    def arrive(self, slot, half=None):
        if half is None:
            ref, sem = self.buf.at[slot], self.recv.at[slot, 0]
        else:
            ref, sem = self.part(slot, half), self.recv.at[slot, half]
        pltpu.make_async_copy(ref, ref, sem).wait()

    def begin(self):
        tp, sibling, right, left, far = ring()
        self.count = 0
        self.push(self.own, tp, right)
        self.push(self.own, tp, left)
        self.push(self.own, tp, sibling)

    def stage(self, n):
        tp, sibling, right, left, far = ring()
        self.count = 3 + 2 * n
        if n == 0:
            self.arrive(left)
            self.push(self.part(left, 0), left, right, 0)
            self.push(self.buf.at[left], left, sibling)
        elif n == 1:
            self.arrive(right)
            self.push(self.part(right, 1), right, left, 1)
            self.push(self.buf.at[right], right, sibling)
        else:
            for half in range(2):
                self.arrive(far, half)
                self.push(self.part(far, half), far, sibling, half)

    def relay(self):
        for n in range(3):
            self.stage(n)

    def finish(self):
        tp, sibling, right, left, far = ring()
        x = tp // 2
        other = 1 - tp % 2
        self.arrive(sibling)
        self.arrive(((x + 3) % 4) * 2 + other)
        self.arrive(((x + 1) % 4) * 2 + other)
        for half in range(2):
            self.arrive(((x + 2) % 4) * 2 + other, half)

    def sent(self):
        for n in range(9):
            ref = self.own if n not in (3, 5, 7, 8) else self.part(0, 0)
            pltpu.make_async_copy(ref, ref, self.send.at[n]).wait()


def greet_all():
    me = lax.axis_index("sp")
    tp = lax.axis_index("tp")
    barrier = pltpu.get_barrier_semaphore()

    def one(i, _):
        sp = (me + i // 8) % 16
        to = (tp + i % 8) % 8
        pl.semaphore_signal(
            barrier, inc=1, device_id={"sp": sp, "tp": to}, device_id_type=MESH
        )
        return 0

    lax.fori_loop(1, 128, one, 0)


class GridGather:
    def __init__(self, buf, send, recv):
        self.buf, self.send, self.recv = buf, send, recv

    def view(self, phase, part, k, half=None):
        me = lax.axis_index("sp")
        z, y = me // 4, me % 4
        tail = (part,) if half is None else (part, half)
        if phase == 0:
            return self.buf.at[(z, k) + tail] if part == 0 else self.buf.at[(k, y) + tail]
        every = pl.ds(0, 4)
        return self.buf.at[(k, every) + tail] if part == 0 else self.buf.at[(every, k) + tail]

    def ring(self, phase, part):
        me = lax.axis_index("sp")
        z, y = me // 4, me % 4
        along_y = phase == part
        at = y if along_y else z
        right, left = (at + 1) % 4, (at + 3) % 4
        if along_y:
            return at, right, left, z * 4 + right, z * 4 + left
        return at, right, left, right * 4 + y, left * 4 + y

    def copies(self, phase, part):
        at, right, left, to_right, to_left = self.ring(phase, part)

        def one(n, view, to):
            return pltpu.make_async_remote_copy(
                src_ref=view,
                dst_ref=view,
                send_sem=self.send.at[phase, part, n],
                recv_sem=self.recv.at[phase, part, n],
                device_id={"sp": to},
                device_id_type=MESH,
            )

        return (
            one(0, self.view(phase, part, at), to_right),
            one(1, self.view(phase, part, at), to_left),
            one(2, self.view(phase, part, left, 0), to_right),
            one(3, self.view(phase, part, right, 1), to_left),
        )

    def begin(self, phase):
        for part in range(2):
            copies = self.copies(phase, part)
            copies[0].start()
            copies[1].start()

    def relay(self, phase):
        for part in range(2):
            copies = self.copies(phase, part)
            copies[0].wait_recv()
            copies[2].start()
            copies[1].wait_recv()
            copies[3].start()

    def finish(self, phase):
        for part in range(2):
            copies = self.copies(phase, part)
            copies[2].wait_recv()
            copies[3].wait_recv()

    def sent(self):
        for phase in range(2):
            for part in range(2):
                for copy in self.copies(phase, part):
                    copy.wait_send()


def layer_kernel(
    q_hbm, k_hbm, v_hbm, g_ref, w_ref, stream, gate_w, up_w, down_w, gain1, bias1, gain2, bias2,
    out,
    q_ref, k_ref, v_ref, att, wall, kvl, qt, ksrc, qsrc, X, R, S0, S1, mx0, mx1, M, A, O,
    G, D, rows, lhs, res, hid, pb, sib, zz, rel, inn,
    ks, kr, qs, qr, ws, wr, ld, gs, gr, Gs, Gr, Ds, Dr, ns, nr, ss, sr, hs, hr,
):
    me = lax.axis_index("sp")
    tp = lax.axis_index("tp")
    z, y = me // 4, me % 4
    greet_all()
    loads = [
        pltpu.make_async_copy(src, dst, ld.at[n])
        for n, (src, dst) in enumerate(
            (
                (k_hbm, k_ref),
                (v_hbm, v_ref),
                (q_hbm, q_ref),
                (w_ref, wall.at[tp]),
                (gate_w, G.at[z, y, :, 0]),
                (up_w, G.at[z, y, :, 1]),
                (down_w, D.at[z, y]),
                (stream.at[pl.ds(pl.multiple_of(tp * 96, 96), 96)], res),
            )
        )
    ]
    for load in loads:
        load.start()
    for load in loads[:3]:
        load.wait()
    kt = k_ref[...].T
    vt = v_ref[...].T
    qtt = q_ref[...].T
    gates = g_ref[...]
    row = lax.broadcasted_iota(jnp.int32, (16, BL), 0)
    for h in range(4):
        g = gates[h : h + 1]
        first = jnp.broadcast_to(g[:, 0:1], (1, BL))
        lines = [jnp.ones((1, BL), jnp.float32)]
        lines += parts((first - g) * LOG2E) + parts(first * (-LOG2E))
        extra = jnp.zeros((16, BL), jnp.float32)
        for n, r in enumerate(lines):
            extra = jnp.where(row == n, r, extra)
        ksrc[h, 0:64] = kt[64 * h : 64 * h + 64]
        ksrc[h, 64:80] = extra.astype(jnp.bfloat16)
        ksrc[h, 80:144] = vt[64 * h : 64 * h + 64]
        for i in range(3):
            qsrc[3 * h + i] = qtt[64 * h : 64 * h + 64, 256 * i : 256 * i + 256]
    pl.semaphore_wait(pltpu.get_barrier_semaphore(), 127)
    qsends = []
    for h in range(4):
        for i in range(3):
            n = 3 * h + i
            sub = 3 * me + i
            c, u = sub // 2, sub % 2
            r = c % 8
            high = r // 4
            member = r + high * (7 - 2 * r)
            slot = 2 * ((c // 8) * 2 + high) + u
            to = place_of(h, member)
            copy = pltpu.make_async_remote_copy(
                src_ref=qsrc.at[n],
                dst_ref=qt.at[slot],
                send_sem=qs.at[n],
                recv_sem=qr.at[slot],
                device_id={"sp": to},
                device_id_type=MESH,
            )
            local = pltpu.make_async_copy(qsrc.at[n], qt.at[slot], qr.at[slot])

            @pl.when(to != me)
            def _():
                copy.start()

            @pl.when(to == me)
            def _():
                local.start()

            qsends.append((to, copy))
    sends = []
    for o in ORDER:
        to = ((z + o // 4) % 4) * 4 + (y + o % 4) % 4
        copy = pltpu.make_async_remote_copy(
            src_ref=ksrc.at[head_of(to)],
            dst_ref=kvl.at[me],
            send_sem=ks.at[o],
            recv_sem=kr.at[me],
            device_id={"sp": to},
            device_id_type=MESH,
        )
        copy.start()
        sends.append(copy)
    own = pltpu.make_async_copy(ksrc.at[head_of(me)], kvl.at[me], kr.at[me])
    own.start()
    for load in loads[3:]:
        load.wait()
    gather = RingGather(wall.at[tp], wall, ws, wr)
    gather.begin()
    upper = GridGather(G, Gs, Gr)
    lower = GridGather(D, Ds, Dr)
    upper.begin(0)
    lower.begin(0)

    row = lax.broadcasted_iota(jnp.int32, (64, QW), 0)
    ones = jnp.where((row >= 1) & (row < 4), 1.0, 0.0).astype(jnp.bfloat16)
    for t in range(NT):
        for u in range(2):
            pltpu.make_async_copy(qsrc.at[0], qt.at[2 * t + u], qr.at[2 * t + u]).wait()
        q = jnp.concatenate([qt[2 * t], qt[2 * t + 1]], axis=1).astype(jnp.float32)
        q = q * (LOG2E / 8)
        hi = q.astype(jnp.bfloat16)
        R[t, 0:64] = hi
        R[t, 64:128] = ones
        R[t, 128:192] = (q - hi.astype(jnp.float32)).astype(jnp.bfloat16)
        R[t, 192:256] = jnp.zeros((64, QW), jnp.bfloat16)
        M[t] = jnp.full((8, QW), NEG, jnp.float32)
        A[t] = jnp.zeros((80, QW), jnp.float32)

    mm = member_of(me)
    S = (S0, S1)
    mx = (mx0, mx1)

    def qk(t, n):
        x = X[...]
        s = jnp.dot(
            jnp.concatenate([x, x], axis=1), R[t], preferred_element_type=jnp.float32
        )
        S[n][...] = s
        mx[n][...] = jnp.max(s.reshape(BL // 8, 8, QW), axis=0)

    def mask(b, t, n):
        c = chunk_of(t, mm)

        @pl.when(b * BL + BL > c * QW)
        def _():
            kp = b * BL + lax.broadcasted_iota(jnp.int32, (BL, QW), 0)
            qp = c * QW + lax.broadcasted_iota(jnp.int32, (BL, QW), 1)
            s = jnp.where(kp <= qp, S[n][...], NEG)
            S[n][...] = s
            mx[n][...] = jnp.max(s.reshape(BL // 8, 8, QW), axis=0)

    def pv(b, t, n, bs):
        m_old = M[t][0:1]
        m_new = jnp.maximum(m_old, jnp.max(mx[n][...], axis=0, keepdims=True) + bs)
        p = jnp.exp2(S[n][...] - (m_new - bs)).astype(jnp.bfloat16)
        o = jnp.dot(kvl[b, 64:144], p, preferred_element_type=jnp.float32)
        A[t] = A[t] * jnp.exp2(m_old - m_new) + o
        M[t] = jnp.broadcast_to(m_new, (8, QW))

    def block(i, _):
        o = i
        b = ((z + 4 - o // 4) % 4) * 4 + (y + 4 - o % 4) % 4
        pltpu.make_async_copy(ksrc.at[0], kvl.at[b], kr.at[b]).wait()
        X[...] = kvl[b, 0:128, :].T
        g = kvl[b, 64:80, 0:128].astype(jnp.float32)
        bs = jnp.tile(g[4:5] + g[5:6] + g[6:7], (1, QW // 128))

        def live(t):
            return chunk_of(t, mm) * QW + QW > b * BL

        for t in range(NT):
            first = live(t) if t == 0 else live(t) & jnp.logical_not(live(t - 1))

            @pl.when(first)
            def _():
                qk(t, t % 2)
                mask(b, t, t % 2)

            @pl.when(live(t))
            def _():
                if t + 1 < NT:
                    qk(t + 1, (t + 1) % 2)
                pv(b, t, t % 2, bs)
                if t + 1 < NT:
                    mask(b, t + 1, (t + 1) % 2)

        for stage in range(3):

            @pl.when(i == RELAY[stage])
            def _():
                gather.stage(stage)

        return 0

    lax.fori_loop(0, 16, block, 0)

    head = tp * 4 + head_of(me)

    def piece(t, u, w):
        sub = 2 * chunk_of(t, mm) + u
        n = 8 * (sub % 3) + w
        to_sp, to_tp, spot = sub // 3, n // 3, n % 3
        src = O.at[(2 * t + u) * 8 + w]
        dst = att.at[head, spot]
        copy = pltpu.make_async_remote_copy(
            src_ref=src,
            dst_ref=dst,
            send_sem=gs.at[(2 * t + u) * 8 + w],
            recv_sem=gr,
            device_id={"sp": to_sp, "tp": to_tp},
            device_id_type=MESH,
        )
        return (to_sp == me) & (to_tp == tp), copy, src, dst

    for t in range(NT):
        a = A[t]
        heads = (a[16:80] / a[0:1]).T.astype(jnp.bfloat16)
        for n in range(16):
            O[16 * t + n] = jnp.concatenate(
                [heads[32 * n : 32 * n + 16], heads[32 * n + 16 : 32 * n + 32]], axis=1
            )
    for t in range(NT):
        for u in range(2):

            def send(w, _):
                mine, copy, src, dst = piece(t, u, w)

                @pl.when(jnp.logical_not(mine))
                def _():
                    copy.start()

                @pl.when(mine)
                def _():
                    pltpu.make_async_copy(src, dst, gr).start()

                return 0

            lax.fori_loop(0, 8, send, 0)
    upper.relay(0)
    lower.relay(0)
    upper.finish(0)
    upper.begin(1)
    lower.finish(0)
    lower.begin(1)
    gather.finish()
    pltpu.make_async_copy(att, att, gr).wait()
    for h in range(32):
        for n in range(3):
            lhs[32 * n : 32 * n + 16, HD * h : HD * h + HD] = att[h, n, :, 0:64]
            lhs[32 * n + 16 : 32 * n + 32, HD * h : HD * h + HD] = att[h, n, :, 64:128]
    mixed = jnp.dot(
        lhs[...], wall[...].reshape(2048, 2048), preferred_element_type=jnp.float32
    )
    mixed = mixed.astype(jnp.bfloat16).astype(jnp.float32)
    p = ALPHA * res[...].astype(jnp.float32) + mixed
    rows[tp] = layer_norm(p, gain1[...], bias1[...]).astype(jnp.bfloat16)
    spread = RingGather(rows.at[tp], rows, ns, nr)
    spread.begin()
    upper.relay(1)

    x, core = tp // 2, tp % 2
    _, sibling, right, left, far = ring()

    def project(chip):
        r = rows[pl.ds(2 * chip, 2)].reshape(192, 2048)
        gate = jnp.dot(
            r, G[:, :, :, 0].reshape(2048, 704), preferred_element_type=jnp.float32
        )
        up = jnp.dot(
            r, G[:, :, :, 1].reshape(2048, 704), preferred_element_type=jnp.float32
        )
        hid[chip] = (gate / (1.0 + jnp.exp(-gate)) * up).astype(jnp.bfloat16)

    other = 1 - core
    spread.stage(0)
    spread.stage(1)
    upper.finish(1)
    lower.relay(1)
    spread.arrive(sibling)
    chips = ((x + 2) % 4, (x + 1) % 4, (x + 3) % 4, x)

    def early(n, _):
        chip = (x + n - n // 2 + n % 2 * (1 - n // 2) * 2) % 4
        project(chip)

        @pl.when(n == 0)
        def _():
            spread.stage(2)
            spread.arrive(chips[2] * 2 + other)
            spread.arrive(chips[1] * 2 + other)

        @pl.when(n == 2)
        def _():
            for half in range(2):
                spread.arrive(chips[0] * 2 + other, half)

        return 0

    lax.fori_loop(0, 4, early, 0)
    lower.finish(1)

    def to_sibling(n):
        return pltpu.make_async_remote_copy(
            src_ref=pb.at[n, other],
            dst_ref=sib.at[n],
            send_sem=ss.at[n],
            recv_sem=sr.at[n],
            device_id={"tp": sibling},
            device_id_type=MESH,
        )

    def hop(n, src, dst, peer):
        return pltpu.make_async_remote_copy(
            src_ref=src,
            dst_ref=dst,
            send_sem=hs.at[n],
            recv_sem=hr.at[n],
            device_id={"tp": peer},
            device_id_type=MESH,
        )

    hops = [
        hop(0, zz.at[0, pl.ds(0, 48)], rel.at[0], right),
        hop(1, zz.at[0, pl.ds(48, 48)], rel.at[1], left),
        hop(2, zz.at[1], inn.at[0], right),
        hop(3, zz.at[2], inn.at[1], left),
    ]

    def product(n):
        wd = jnp.concatenate(
            [D[k // 4, k % 4].reshape(704, 128) for k in range(16)], axis=1
        )
        s = jnp.dot(hid[chips[n]], wd, preferred_element_type=jnp.float32)
        s = s.astype(jnp.bfloat16)
        pb[n, 0] = s[:96]
        pb[n, 1] = s[96:]
        to_sibling(n).start()

    def pair(n):
        to_sibling(n).wait_recv()
        return pb[n, core].astype(jnp.float32) + sib[n].astype(jnp.float32)

    product(0)
    product(1)
    zz[0] = pair(0).astype(jnp.bfloat16)
    hops[0].start()
    hops[1].start()
    product(2)
    s = pair(1)
    hops[0].wait_recv()
    zz[1, 0:48] = (s[:48] + rel[0].astype(jnp.float32)).astype(jnp.bfloat16)
    zz[1, 48:96] = s[48:].astype(jnp.bfloat16)
    hops[2].start()
    product(3)
    s = pair(2)
    hops[1].wait_recv()
    zz[2, 0:48] = s[:48].astype(jnp.bfloat16)
    zz[2, 48:96] = (s[48:] + rel[1].astype(jnp.float32)).astype(jnp.bfloat16)
    hops[3].start()
    s = pair(3)
    hops[2].wait_recv()
    hops[3].wait_recv()
    s = s + inn[0].astype(jnp.float32) + inn[1].astype(jnp.float32)
    lowered = s.astype(jnp.bfloat16).astype(jnp.float32)
    normed = rows[tp].astype(jnp.float32)
    out[...] = layer_norm(ALPHA * normed + lowered, gain2[...], bias2[...]).astype(jnp.bfloat16)
    for n in range(4):
        to_sibling(n).wait_send()
        hops[n].wait_send()
    spread.sent()
    upper.sent()
    lower.sent()
    for t in range(NT):
        for u in range(2):

            def sent(w, _):
                mine, copy, src, dst = piece(t, u, w)

                @pl.when(jnp.logical_not(mine))
                def _():
                    copy.wait_send()

                return 0

            lax.fori_loop(0, 8, sent, 0)
    gather.sent()
    for copy in sends:
        copy.wait_send()
    for to, copy in qsends:

        @pl.when(to != me)
        def _():
            copy.wait_send()


def layer(*args):
    bf = jnp.bfloat16
    dma = pltpu.SemaphoreType.DMA
    scratch = [
        pltpu.VMEM((BL, 256), bf),
        pltpu.VMEM((BL, 256), bf),
        pltpu.VMEM((BL, 256), bf),
        pltpu.VMEM((32, 3, 16, 128), bf),
        pltpu.VMEM((8, 256, 2048), bf),
        pltpu.VMEM((NB, KVR, BL), bf),
        pltpu.VMEM((2 * NT, HD, 256), bf),
        pltpu.VMEM((4, KVR, BL), bf),
        pltpu.VMEM((12, HD, 256), bf),
        pltpu.VMEM((BL, 128), bf),
        pltpu.VMEM((NT, 256, QW), bf),
        pltpu.VMEM((BL, QW), jnp.float32),
        pltpu.VMEM((BL, QW), jnp.float32),
        pltpu.VMEM((8, QW), jnp.float32),
        pltpu.VMEM((8, QW), jnp.float32),
        pltpu.VMEM((NT, 8, QW), jnp.float32),
        pltpu.VMEM((NT, 80, QW), jnp.float32),
        pltpu.VMEM((96, 16, 128), bf),
        pltpu.VMEM((4, 4, 2, 2, 64, 704), bf),
        pltpu.VMEM((4, 4, 2, 2, 176, 128), bf),
        pltpu.VMEM((8, 96, 2048), bf),
        pltpu.VMEM((96, 2048), bf),
        pltpu.VMEM((96, 2048), bf),
        pltpu.VMEM((4, 192, 704), bf),
        pltpu.VMEM((4, 2, 96, 2048), bf),
        pltpu.VMEM((4, 96, 2048), bf),
        pltpu.VMEM((3, 96, 2048), bf),
        pltpu.VMEM((2, 48, 2048), bf),
        pltpu.VMEM((2, 96, 2048), bf),
        dma((16,)), dma((16,)), dma((12,)), dma((12,)), dma((9,)), dma((8, 2)), dma((8,)),
        dma((96,)), dma, dma((2, 2, 4)), dma((2, 2, 4)), dma((2, 2, 4)), dma((2, 2, 4)),
        dma((9,)), dma((8, 2)), dma((4,)), dma((4,)), dma((4,)), dma((4,)),
    ]
    return pl.pallas_call(
        layer_kernel,
        name="layer",
        out_shape=jax.ShapeDtypeStruct((96, 2048), bf),
        in_specs=[ANY] * 3 + [VMEM] + [ANY] * 5 + [VMEM] * 4,
        out_specs=VMEM,
        scratch_shapes=scratch,
        compiler_params=pltpu.CompilerParams(
            collective_id=0, has_side_effects=True, vmem_limit_bytes=62 * 2**20
        ),
    )(*args)


def body(
    queries,
    key_rows,
    value_rows,
    log_forget,
    stream_in,
    out_weight,
    mix_gain,
    mix_bias,
    gate_weight,
    up_weight,
    down_weight,
    ffn_gain,
    ffn_bias,
):
    return layer(
        queries,
        key_rows,
        value_rows,
        log_forget.T,
        out_weight,
        stream_in,
        gate_weight.reshape(2, 64, 704),
        up_weight.reshape(2, 64, 704),
        down_weight.reshape(2, 2, 176, 128),
        mix_gain[None],
        mix_bias[None],
        ffn_gain[None],
        ffn_bias[None],
    )


def solution(mesh):
    placed = (
        P("sp", "tp"),
        P("sp", "tp"),
        P("sp", "tp"),
        P("sp", "tp"),
        P("sp", None),
        P("tp", None),
        P(),
        P(),
        P("sp", "tp"),
        P("sp", "tp"),
        P("tp", "sp"),
        P(),
        P(),
    )
    return jax.shard_map(
        body, mesh=mesh, in_specs=placed, out_specs=P(("sp", "tp"), None), check_vma=False
    )
```

```python
import functools

import jax
import jax.numpy as jnp
from jax import lax
from jax.experimental import pallas as pl
from jax.experimental.pallas import tpu as pltpu
from jax.sharding import PartitionSpec as P

ALPHA = 8.0**0.25
EPSILON = 1e-05
MESH = pl.DeviceIdType.MESH
LOG2E = 1.4426950408889634
NEG = -1e30
BL = 768
RELAY = (9, 10, 13)
QW = 512
NT = 6
NB = 16
HD = 64
KVR = 144
VMEM = pl.BlockSpec(memory_space=pltpu.VMEM)
ANY = pl.BlockSpec(memory_space=pl.ANY)


def layer_norm(matrix, norm_gain, norm_shift):
    centred = matrix - jnp.mean(matrix, axis=-1, keepdims=True)
    spread = jnp.mean(centred * centred, axis=-1, keepdims=True)
    return centred * lax.rsqrt(spread + EPSILON) * norm_gain + norm_shift


def parts(x):
    hi = x.astype(jnp.bfloat16).astype(jnp.float32)
    rest = x - hi
    mid = rest.astype(jnp.bfloat16).astype(jnp.float32)
    return hi, mid, rest - mid


def head_of(sp):
    z, y = sp // 4, sp % 4
    return (z // 2) * 2 + y // 2


def member_of(sp):
    z, y = sp // 4, sp % 4
    return (z % 2) * 2 + y % 2


def place_of(head, member):
    z = (head // 2) * 2 + member // 2
    y = (head % 2) * 2 + member % 2
    return z * 4 + y


def chunk_of(t, member):
    return (t // 2) * 8 + (member if t % 2 == 0 else 7 - member)


def ring():
    tp = lax.axis_index("tp")
    x, core = tp // 2, tp % 2
    right = ((x + 1) % 4) * 2 + core
    left = ((x + 3) % 4) * 2 + core
    far = ((x + 2) % 4) * 2 + core
    return tp, x * 2 + 1 - core, right, left, far


def greet_ring():
    tp, sibling, right, left, far = ring()
    barrier = pltpu.get_barrier_semaphore()
    for peer in (sibling, right, left):
        pl.semaphore_signal(barrier, inc=1, device_id={"tp": peer}, device_id_type=MESH)


class RingGather:
    def __init__(self, own, buf, send, recv):
        self.own, self.buf, self.send, self.recv = own, buf, send, recv
        self.rows = buf.shape[1]
        self.half = self.rows // 2
        self.count = 0

    def push(self, src, slot, peer, half=None):
        if half is None:
            dst, sem = self.buf.at[slot], self.recv.at[slot, 0]
        else:
            cut = pl.ds(half * self.half, self.half)
            dst, sem = self.buf.at[slot, cut], self.recv.at[slot, half]
        copy = pltpu.make_async_remote_copy(
            src_ref=src,
            dst_ref=dst,
            send_sem=self.send.at[self.count],
            recv_sem=sem,
            device_id={"tp": peer},
            device_id_type=MESH,
        )
        copy.start()
        self.count += 1

    def part(self, slot, half):
        return self.buf.at[slot, pl.ds(half * self.half, self.half)]

    def arrive(self, slot, half=None):
        if half is None:
            ref, sem = self.buf.at[slot], self.recv.at[slot, 0]
        else:
            ref, sem = self.part(slot, half), self.recv.at[slot, half]
        pltpu.make_async_copy(ref, ref, sem).wait()

    def begin(self):
        tp, sibling, right, left, far = ring()
        self.count = 0
        self.push(self.own, tp, right)
        self.push(self.own, tp, left)
        self.push(self.own, tp, sibling)

    def stage(self, n):
        tp, sibling, right, left, far = ring()
        self.count = 3 + 2 * n
        if n == 0:
            self.arrive(left)
            self.push(self.part(left, 0), left, right, 0)
            self.push(self.buf.at[left], left, sibling)
        elif n == 1:
            self.arrive(right)
            self.push(self.part(right, 1), right, left, 1)
            self.push(self.buf.at[right], right, sibling)
        else:
            for half in range(2):
                self.arrive(far, half)
                self.push(self.part(far, half), far, sibling, half)

    def relay(self):
        for n in range(3):
            self.stage(n)

    def finish(self):
        tp, sibling, right, left, far = ring()
        x = tp // 2
        other = 1 - tp % 2
        self.arrive(sibling)
        self.arrive(((x + 3) % 4) * 2 + other)
        self.arrive(((x + 1) % 4) * 2 + other)
        for half in range(2):
            self.arrive(((x + 2) % 4) * 2 + other, half)

    def sent(self):
        for n in range(9):
            ref = self.own if n not in (3, 5, 7, 8) else self.part(0, 0)
            pltpu.make_async_copy(ref, ref, self.send.at[n]).wait()


def greet_lines():
    me = lax.axis_index("sp")
    tp = lax.axis_index("tp")
    barrier = pltpu.get_barrier_semaphore()
    for n in range(1, 16):
        to = (me + n) % 16
        pl.semaphore_signal(barrier, inc=1, device_id={"sp": to}, device_id_type=MESH)
    for n in range(1, 8):
        to = (tp + n) % 8
        pl.semaphore_signal(barrier, inc=1, device_id={"tp": to}, device_id_type=MESH)


class GridGather:
    def __init__(self, buf, send, recv):
        self.buf, self.send, self.recv = buf, send, recv

    def view(self, phase, part, k, half=None):
        me = lax.axis_index("sp")
        z, y = me // 4, me % 4
        tail = (part,) if half is None else (part, half)
        if phase == 0:
            return self.buf.at[(z, k) + tail] if part == 0 else self.buf.at[(k, y) + tail]
        every = pl.ds(0, 4)
        return self.buf.at[(k, every) + tail] if part == 0 else self.buf.at[(every, k) + tail]

    def ring(self, phase, part):
        me = lax.axis_index("sp")
        z, y = me // 4, me % 4
        along_y = phase == part
        at = y if along_y else z
        right, left = (at + 1) % 4, (at + 3) % 4
        if along_y:
            return at, right, left, z * 4 + right, z * 4 + left
        return at, right, left, right * 4 + y, left * 4 + y

    def copies(self, phase, part):
        at, right, left, to_right, to_left = self.ring(phase, part)

        def one(n, view, to):
            return pltpu.make_async_remote_copy(
                src_ref=view,
                dst_ref=view,
                send_sem=self.send.at[phase, part, n],
                recv_sem=self.recv.at[phase, part, n],
                device_id={"sp": to},
                device_id_type=MESH,
            )

        return (
            one(0, self.view(phase, part, at), to_right),
            one(1, self.view(phase, part, at), to_left),
            one(2, self.view(phase, part, left, 0), to_right),
            one(3, self.view(phase, part, right, 1), to_left),
        )

    def begin(self, phase):
        for part in range(2):
            copies = self.copies(phase, part)
            copies[0].start()
            copies[1].start()

    def relay(self, phase):
        for part in range(2):
            copies = self.copies(phase, part)
            copies[0].wait_recv()
            copies[2].start()
            copies[1].wait_recv()
            copies[3].start()

    def finish(self, phase):
        for part in range(2):
            copies = self.copies(phase, part)
            copies[2].wait_recv()
            copies[3].wait_recv()

    def sent(self):
        for phase in range(2):
            for part in range(2):
                for copy in self.copies(phase, part):
                    copy.wait_send()


def layer_kernel(
    q_hbm, k_hbm, v_hbm, g_ref, w_ref, stream, gate_w, up_w, down_w, gain1, bias1, gain2, bias2,
    out,
    q_ref, k_ref, v_ref, att, wall, kvl, qt, ksrc, qsrc, X, R, S0, S1, mx0, mx1, M, A, O,
    G, D, rows, lhs, res, hid, pb, sib, zz, rel, inn, E, gt,
    ks, kr, qs, qr, ws, wr, ld, gs, gr, Gs, Gr, Ds, Dr, ns, nr, ss, sr, hs, hr, er, line,
):
    me = lax.axis_index("sp")
    tp = lax.axis_index("tp")
    z, y = me // 4, me % 4
    greet_lines()
    loads = [
        pltpu.make_async_copy(src, dst, ld.at[n])
        for n, (src, dst) in enumerate(
            (
                (k_hbm, k_ref),
                (v_hbm, v_ref),
                (q_hbm, q_ref),
                (w_ref, wall.at[tp]),
                (gate_w, gt.at[0]),
                (up_w, gt.at[1]),
                (down_w.at[pl.ds(0, 176)], D.at[z, y, 0, 0]),
                (down_w.at[pl.ds(176, 176)], D.at[z, y, 0, 1]),
                (down_w.at[pl.ds(352, 176)], D.at[z, y, 1, 0]),
                (down_w.at[pl.ds(528, 176)], D.at[z, y, 1, 1]),
                (stream.at[pl.ds(pl.multiple_of(tp * 96, 96), 96)], res),
            )
        )
    ]
    for load in loads:
        load.start()
    for load in loads[:3]:
        load.wait()
    kt = k_ref[...].T
    vt = v_ref[...].T
    qtt = q_ref[...].T
    gates = g_ref[...]
    row = lax.broadcasted_iota(jnp.int32, (16, BL), 0)
    for h in range(4):
        g = gates[h : h + 1]
        first = jnp.broadcast_to(g[:, 0:1], (1, BL))
        lines = [jnp.ones((1, BL), jnp.float32)]
        lines += parts((first - g) * LOG2E) + parts(first * (-LOG2E))
        extra = jnp.zeros((16, BL), jnp.float32)
        for n, r in enumerate(lines):
            extra = jnp.where(row == n, r, extra)
        ksrc[h, 0:64] = kt[64 * h : 64 * h + 64]
        ksrc[h, 64:80] = extra.astype(jnp.bfloat16)
        ksrc[h, 80:144] = vt[64 * h : 64 * h + 64]
        for i in range(3):
            qsrc[3 * h + i] = qtt[64 * h : 64 * h + 64, 256 * i : 256 * i + 256]
    pl.semaphore_wait(pltpu.get_barrier_semaphore(), 22)
    for n in range(1, 16):
        to = (me + n) % 16
        pl.semaphore_signal(line, inc=1, device_id={"sp": to}, device_id_type=MESH)
    qsends = []
    for h in range(4):
        for i in range(3):
            n = 3 * h + i
            sub = 3 * me + i
            c, u = sub // 2, sub % 2
            r = c % 8
            high = r // 4
            member = r + high * (7 - 2 * r)
            slot = 2 * ((c // 8) * 2 + high) + u
            to = place_of(h, member)
            copy = pltpu.make_async_remote_copy(
                src_ref=qsrc.at[n],
                dst_ref=qt.at[slot],
                send_sem=qs.at[n],
                recv_sem=qr.at[slot],
                device_id={"sp": to},
                device_id_type=MESH,
            )
            local = pltpu.make_async_copy(qsrc.at[n], qt.at[slot], qr.at[slot])

            @pl.when(to != me)
            def _():
                copy.start()

            @pl.when(to == me)
            def _():
                local.start()

            qsends.append((to, copy))
    own = pltpu.make_async_copy(ksrc.at[head_of(me)], kvl.at[me], kr.at[me])
    own.start()
    par = (z + y) % 2

    def axes(cls):
        return y + cls * (z - y), z + cls * (y - z)

    def dev(cls, a, c):
        return a * (1 + 3 * cls) + c * (4 - 3 * cls)

    def half_head(cls, a, c):
        return a * (1 + cls) + c * (2 - cls)

    def mate(k):
        return k + 1 - 2 * (k % 2)

    def pass_on(n, src, dst, sem, to):
        return pltpu.make_async_remote_copy(
            src_ref=src,
            dst_ref=dst,
            send_sem=ks.at[n],
            recv_sem=sem,
            device_id={"sp": to},
            device_id_type=MESH,
        )

    a, c = axes(par)
    ap, cp = a // 2, c // 2
    mine = (kvl.at[me], kr.at[me])
    side = (E.at[par, a], er.at[par, a])
    for n, (head, (dst, sem), to) in enumerate(
        (
            (half_head(par, 1 - ap, 1 - cp), side, dev(par, 3 - a, c)),
            (half_head(par, ap, 1 - cp), side, dev(par, mate(a), c)),
            (half_head(par, 1 - ap, cp), mine, dev(par, 3 - a, c)),
            (half_head(par, ap, cp), mine, dev(par, mate(a), c)),
            (half_head(par, ap, 1 - cp), mine, dev(par, a, 3 - c)),
            (half_head(par, ap, cp), mine, dev(par, a, mate(c))),
        )
    ):
        pass_on(n, ksrc.at[head], dst, sem, to).start()

    def fan(n, cls, b, slot):
        a, c = axes(cls)
        pltpu.make_async_copy(E.at[cls, slot], E.at[cls, slot], er.at[cls, slot]).wait()
        pass_on(n, E.at[cls, slot], kvl.at[b], kr.at[b], dev(cls, a, 3 - c)).start()
        pass_on(n + 1, kvl.at[b], kvl.at[b], kr.at[b], dev(cls, a, mate(c))).start()

    def order(i):
        j = jnp.maximum(i - 4, 0)
        g, cls, f = j // 4, j % 4 // 2, j % 2
        a, c = axes(cls)
        far_c = jnp.where(g == 0, 3 - c, jnp.where(g == 1, mate(c), (c + 2) % 4))
        late = dev(cls, (cls + far_c) % 2 + 2 * f, far_c)
        ya, yc = axes(1 - par)
        xa, xc = axes(par)
        early = jnp.where(
            i < 2,
            jnp.where(i == 0, me, dev(1 - par, mate(ya), yc)),
            jnp.where(i == 2, dev(1 - par, 3 - ya, yc), dev(par, (xa + 2) % 4, xc)),
        )
        return jnp.where(i < 4, early, late)

    def arrive(i):
        b = order(i)
        pltpu.make_async_copy(ksrc.at[0], kvl.at[b], kr.at[b]).wait()

        @pl.when(i == 1)
        def _():
            a, c = axes(1 - par)
            fan(6, 1 - par, b, mate(a))

        @pl.when(i == 2)
        def _():
            cls = 1 - par
            a, c = axes(cls)
            slot = 3 - a
            pass_on(8, kvl.at[b], kvl.at[b], kr.at[b], dev(cls, mate(a), c)).start()
            fan(9, cls, b, slot)
            pass_on(
                11, E.at[cls, slot], E.at[cls, slot], er.at[cls, slot], dev(cls, mate(a), c)
            ).start()

        @pl.when(i == 3)
        def _():
            a, c = axes(par)
            fan(12, par, b, (a + 2) % 4)

        @pl.when((i >= 4) & (i < 8))
        def _():
            cls = (i - 4) // 2
            a, c = axes(cls)
            pass_on(10 + i, kvl.at[b], kvl.at[b], kr.at[b], dev(cls, a, mate(c))).start()

    for load in loads[3:]:
        load.wait()
    gather = RingGather(wall.at[tp], wall, ws, wr)
    gather.begin()
    for n in range(2):
        turned = gt[n].T
        for half in range(2):
            G[z, y, half, n] = turned[64 * half : 64 * half + 64]
    upper = GridGather(G, Gs, Gr)
    lower = GridGather(D, Ds, Dr)
    upper.begin(0)
    lower.begin(0)

    row = lax.broadcasted_iota(jnp.int32, (64, QW), 0)
    ones = jnp.where((row >= 1) & (row < 4), 1.0, 0.0).astype(jnp.bfloat16)
    for t in range(NT):
        for u in range(2):
            pltpu.make_async_copy(qsrc.at[0], qt.at[2 * t + u], qr.at[2 * t + u]).wait()
        q = jnp.concatenate([qt[2 * t], qt[2 * t + 1]], axis=1).astype(jnp.float32)
        q = q * (LOG2E / 8)
        hi = q.astype(jnp.bfloat16)
        R[t, 0:64] = hi
        R[t, 64:128] = ones
        R[t, 128:192] = (q - hi.astype(jnp.float32)).astype(jnp.bfloat16)
        R[t, 192:256] = jnp.zeros((64, QW), jnp.bfloat16)
        M[t] = jnp.full((8, QW), NEG, jnp.float32)
        A[t] = jnp.zeros((80, QW), jnp.float32)

    mm = member_of(me)
    S = (S0, S1)
    mx = (mx0, mx1)

    def qk(t, n):
        x = X[...]
        s = jnp.dot(
            jnp.concatenate([x, x], axis=1), R[t], preferred_element_type=jnp.float32
        )
        S[n][...] = s
        mx[n][...] = jnp.max(s.reshape(BL // 8, 8, QW), axis=0)

    def mask(b, t, n):
        c = chunk_of(t, mm)

        @pl.when(b * BL + BL > c * QW)
        def _():
            kp = b * BL + lax.broadcasted_iota(jnp.int32, (BL, QW), 0)
            qp = c * QW + lax.broadcasted_iota(jnp.int32, (BL, QW), 1)
            s = jnp.where(kp <= qp, S[n][...], NEG)
            S[n][...] = s
            mx[n][...] = jnp.max(s.reshape(BL // 8, 8, QW), axis=0)

    def pv(b, t, n, bs):
        m_old = M[t][0:1]
        m_new = jnp.maximum(m_old, jnp.max(mx[n][...], axis=0, keepdims=True) + bs)
        p = jnp.exp2(S[n][...] - (m_new - bs)).astype(jnp.bfloat16)
        o = jnp.dot(kvl[b, 64:144], p, preferred_element_type=jnp.float32)
        A[t] = A[t] * jnp.exp2(m_old - m_new) + o
        M[t] = jnp.broadcast_to(m_new, (8, QW))

    def block(i, _):
        b = order(i)

        @pl.when(i < 14)
        def _():
            arrive(i + 2)

        X[...] = kvl[b, 0:128, :].T
        g = kvl[b, 64:80, 0:128].astype(jnp.float32)
        bs = jnp.tile(g[4:5] + g[5:6] + g[6:7], (1, QW // 128))

        def live(t):
            return chunk_of(t, mm) * QW + QW > b * BL

        for t in range(NT):
            first = live(t) if t == 0 else live(t) & jnp.logical_not(live(t - 1))

            @pl.when(first)
            def _():
                qk(t, t % 2)
                mask(b, t, t % 2)

            @pl.when(live(t))
            def _():
                if t + 1 < NT:
                    qk(t + 1, (t + 1) % 2)
                pv(b, t, t % 2, bs)
                if t + 1 < NT:
                    mask(b, t + 1, (t + 1) % 2)

        for stage in range(3):

            @pl.when(i == RELAY[stage])
            def _():
                gather.stage(stage)

        @pl.when(i == 6)
        def _():
            upper.relay(0)
            lower.relay(0)

        @pl.when(i == 8)
        def _():
            upper.finish(0)
            upper.begin(1)
            lower.finish(0)
            lower.begin(1)

        return 0

    arrive(0)
    arrive(1)
    lax.fori_loop(0, 16, block, 0)

    head = tp * 4 + head_of(me)

    def piece(t, u, w):
        sub = 2 * chunk_of(t, mm) + u
        n = 8 * (sub % 3) + w
        to_sp, to_tp, spot = sub // 3, n // 3, n % 3
        src = O.at[(2 * t + u) * 8 + w]
        dst = att.at[head, spot]
        copy = pltpu.make_async_remote_copy(
            src_ref=src,
            dst_ref=dst,
            send_sem=gs.at[(2 * t + u) * 8 + w],
            recv_sem=gr,
            device_id={"sp": to_sp, "tp": to_tp},
            device_id_type=MESH,
        )
        return (to_sp == me) & (to_tp == tp), copy, src, dst

    for t in range(NT):
        a = A[t]
        heads = (a[16:80] / a[0:1]).T.astype(jnp.bfloat16)
        for n in range(16):
            O[16 * t + n] = jnp.concatenate(
                [heads[32 * n : 32 * n + 16], heads[32 * n + 16 : 32 * n + 32]], axis=1
            )
    pl.semaphore_wait(line, 15)
    for t in range(NT):
        for u in range(2):

            def send(w, _):
                mine, copy, src, dst = piece(t, u, w)

                @pl.when(jnp.logical_not(mine))
                def _():
                    copy.start()

                @pl.when(mine)
                def _():
                    pltpu.make_async_copy(src, dst, gr).start()

                return 0

            lax.fori_loop(0, 8, send, 0)
    upper.relay(1)
    gather.finish()
    pltpu.make_async_copy(att, att, gr).wait()
    for h in range(32):
        for n in range(3):
            lhs[32 * n : 32 * n + 16, HD * h : HD * h + HD] = att[h, n, :, 0:64]
            lhs[32 * n + 16 : 32 * n + 32, HD * h : HD * h + HD] = att[h, n, :, 64:128]
    mixed = jnp.dot(
        lhs[...], wall[...].reshape(2048, 2048), preferred_element_type=jnp.float32
    )
    mixed = mixed.astype(jnp.bfloat16).astype(jnp.float32)
    p = ALPHA * res[...].astype(jnp.float32) + mixed
    rows[tp] = layer_norm(p, gain1[...], bias1[...]).astype(jnp.bfloat16)
    spread = RingGather(rows.at[tp], rows, ns, nr)
    spread.begin()

    x, core = tp // 2, tp % 2
    _, sibling, right, left, far = ring()

    def project(chip):
        r = rows[pl.ds(2 * chip, 2)].reshape(192, 2048)
        gate = jnp.dot(
            r, G[:, :, :, 0].reshape(2048, 704), preferred_element_type=jnp.float32
        )
        up = jnp.dot(
            r, G[:, :, :, 1].reshape(2048, 704), preferred_element_type=jnp.float32
        )
        hid[chip] = (gate / (1.0 + jnp.exp(-gate)) * up).astype(jnp.bfloat16)

    other = 1 - core
    spread.stage(0)
    spread.stage(1)
    upper.finish(1)
    lower.relay(1)
    spread.arrive(sibling)
    chips = ((x + 2) % 4, (x + 1) % 4, (x + 3) % 4, x)

    def early(n, _):
        chip = (x + n - n // 2 + n % 2 * (1 - n // 2) * 2) % 4
        project(chip)

        @pl.when(n == 0)
        def _():
            spread.stage(2)
            spread.arrive(chips[2] * 2 + other)
            spread.arrive(chips[1] * 2 + other)

        @pl.when(n == 2)
        def _():
            for half in range(2):
                spread.arrive(chips[0] * 2 + other, half)

        return 0

    lax.fori_loop(0, 4, early, 0)
    lower.finish(1)

    def to_sibling(n):
        return pltpu.make_async_remote_copy(
            src_ref=pb.at[n, other],
            dst_ref=sib.at[n],
            send_sem=ss.at[n],
            recv_sem=sr.at[n],
            device_id={"tp": sibling},
            device_id_type=MESH,
        )

    def hop(n, src, dst, peer):
        return pltpu.make_async_remote_copy(
            src_ref=src,
            dst_ref=dst,
            send_sem=hs.at[n],
            recv_sem=hr.at[n],
            device_id={"tp": peer},
            device_id_type=MESH,
        )

    hops = [
        hop(0, zz.at[0, pl.ds(0, 48)], rel.at[0], right),
        hop(1, zz.at[0, pl.ds(48, 48)], rel.at[1], left),
        hop(2, zz.at[1], inn.at[0], right),
        hop(3, zz.at[2], inn.at[1], left),
    ]

    def product(n):
        wd = jnp.concatenate(
            [D[k // 4, k % 4].reshape(704, 128) for k in range(16)], axis=1
        )
        s = jnp.dot(hid[chips[n]], wd, preferred_element_type=jnp.float32)
        s = s.astype(jnp.bfloat16)
        pb[n, 0] = s[:96]
        pb[n, 1] = s[96:]
        to_sibling(n).start()

    def pair(n):
        to_sibling(n).wait_recv()
        return pb[n, core].astype(jnp.float32) + sib[n].astype(jnp.float32)

    product(0)
    product(1)
    zz[0] = pair(0).astype(jnp.bfloat16)
    hops[0].start()
    hops[1].start()
    product(2)
    s = pair(1)
    hops[0].wait_recv()
    zz[1, 0:48] = (s[:48] + rel[0].astype(jnp.float32)).astype(jnp.bfloat16)
    zz[1, 48:96] = s[48:].astype(jnp.bfloat16)
    hops[2].start()
    product(3)
    s = pair(2)
    hops[1].wait_recv()
    zz[2, 0:48] = s[:48].astype(jnp.bfloat16)
    zz[2, 48:96] = (s[48:] + rel[1].astype(jnp.float32)).astype(jnp.bfloat16)
    hops[3].start()
    s = pair(3)
    hops[2].wait_recv()
    hops[3].wait_recv()
    s = s + inn[0].astype(jnp.float32) + inn[1].astype(jnp.float32)
    lowered = s.astype(jnp.bfloat16).astype(jnp.float32)
    normed = rows[tp].astype(jnp.float32)
    out[...] = layer_norm(ALPHA * normed + lowered, gain2[...], bias2[...]).astype(jnp.bfloat16)
    for n in range(4):
        to_sibling(n).wait_send()
        hops[n].wait_send()
    spread.sent()
    upper.sent()
    lower.sent()
    for t in range(NT):
        for u in range(2):

            def sent(w, _):
                mine, copy, src, dst = piece(t, u, w)

                @pl.when(jnp.logical_not(mine))
                def _():
                    copy.wait_send()

                return 0

            lax.fori_loop(0, 8, sent, 0)
    gather.sent()
    for n in range(18):
        pltpu.make_async_copy(ksrc.at[0], ksrc.at[0], ks.at[n]).wait()
    for to, copy in qsends:

        @pl.when(to != me)
        def _():
            copy.wait_send()


def layer(*args):
    bf = jnp.bfloat16
    dma = pltpu.SemaphoreType.DMA
    scratch = [
        pltpu.VMEM((BL, 256), bf),
        pltpu.VMEM((BL, 256), bf),
        pltpu.VMEM((BL, 256), bf),
        pltpu.VMEM((32, 3, 16, 128), bf),
        pltpu.VMEM((8, 256, 2048), bf),
        pltpu.VMEM((NB, KVR, BL), bf),
        pltpu.VMEM((2 * NT, HD, 256), bf),
        pltpu.VMEM((4, KVR, BL), bf),
        pltpu.VMEM((12, HD, 256), bf),
        pltpu.VMEM((BL, 128), bf),
        pltpu.VMEM((NT, 256, QW), bf),
        pltpu.VMEM((BL, QW), jnp.float32),
        pltpu.VMEM((BL, QW), jnp.float32),
        pltpu.VMEM((8, QW), jnp.float32),
        pltpu.VMEM((8, QW), jnp.float32),
        pltpu.VMEM((NT, 8, QW), jnp.float32),
        pltpu.VMEM((NT, 80, QW), jnp.float32),
        pltpu.VMEM((96, 16, 128), bf),
        pltpu.VMEM((4, 4, 2, 2, 64, 704), bf),
        pltpu.VMEM((4, 4, 2, 2, 176, 128), bf),
        pltpu.VMEM((8, 96, 2048), bf),
        pltpu.VMEM((96, 2048), bf),
        pltpu.VMEM((96, 2048), bf),
        pltpu.VMEM((4, 192, 704), bf),
        pltpu.VMEM((4, 2, 96, 2048), bf),
        pltpu.VMEM((4, 96, 2048), bf),
        pltpu.VMEM((3, 96, 2048), bf),
        pltpu.VMEM((2, 48, 2048), bf),
        pltpu.VMEM((2, 96, 2048), bf),
        pltpu.VMEM((2, 4, KVR, BL), bf),
        pltpu.VMEM((2, 704, 128), bf),
        dma((18,)), dma((16,)), dma((12,)), dma((12,)), dma((9,)), dma((8, 2)), dma((13,)),
        dma((96,)), dma, dma((2, 2, 4)), dma((2, 2, 4)), dma((2, 2, 4)), dma((2, 2, 4)),
        dma((9,)), dma((8, 2)), dma((4,)), dma((4,)), dma((4,)), dma((4,)), dma((2, 4)),
        pltpu.SemaphoreType.REGULAR,
    ]
    return pl.pallas_call(
        layer_kernel,
        name="layer",
        out_shape=jax.ShapeDtypeStruct((96, 2048), bf),
        in_specs=[ANY] * 3 + [VMEM] + [ANY] * 5 + [VMEM] * 4,
        out_specs=VMEM,
        scratch_shapes=scratch,
        compiler_params=pltpu.CompilerParams(
            collective_id=0, has_side_effects=True, vmem_limit_bytes=62 * 2**20
        ),
    )(*args)


def body(
    queries,
    key_rows,
    value_rows,
    log_forget,
    stream_in,
    out_weight,
    mix_gain,
    mix_bias,
    gate_weight,
    up_weight,
    down_weight,
    ffn_gain,
    ffn_bias,
):
    return layer(
        queries,
        key_rows,
        value_rows,
        log_forget.T,
        out_weight,
        stream_in,
        gate_weight.T,
        up_weight.T,
        down_weight,
        mix_gain[None],
        mix_bias[None],
        ffn_gain[None],
        ffn_bias[None],
    )


def solution(mesh):
    placed = (
        P("sp", "tp"),
        P("sp", "tp"),
        P("sp", "tp"),
        P("sp", "tp"),
        P("sp", None),
        P("tp", None),
        P(),
        P(),
        P("sp", "tp"),
        P("sp", "tp"),
        P("tp", "sp"),
        P(),
        P(),
    )
    return jax.shard_map(
        body, mesh=mesh, in_specs=placed, out_specs=P(("sp", "tp"), None), check_vma=False
    )
```

```python
import functools

import jax
import jax.numpy as jnp
from jax import lax
from jax.experimental import pallas as pl
from jax.experimental.pallas import tpu as pltpu
from jax.sharding import PartitionSpec as P

ALPHA = 8.0**0.25
EPSILON = 1e-05
MESH = pl.DeviceIdType.MESH
LOG2E = 1.4426950408889634
NEG = -1e30
BL = 768
RELAY = (11, 12, 14)
TURNS = (0, 4, 2, 3, 1, 8, 6, 5, 12, 7, 13, 10, 14, 9, 15, 11)
AFTER = (
    (0, (4,)),
    (1, (1, 3, 2)),
    (4, (6, 8)),
    (6, (12, 7, 5)),
    (9, (13, 10)),
    (11, (14, 9)),
    (13, (15,)),
    (14, (11,)),
)
QW = 512
NT = 6
NB = 16
HD = 64
KVR = 144
VMEM = pl.BlockSpec(memory_space=pltpu.VMEM)
ANY = pl.BlockSpec(memory_space=pl.ANY)


def layer_norm(matrix, norm_gain, norm_shift):
    centred = matrix - jnp.mean(matrix, axis=-1, keepdims=True)
    spread = jnp.mean(centred * centred, axis=-1, keepdims=True)
    return centred * lax.rsqrt(spread + EPSILON) * norm_gain + norm_shift


def parts(x):
    hi = x.astype(jnp.bfloat16).astype(jnp.float32)
    rest = x - hi
    mid = rest.astype(jnp.bfloat16).astype(jnp.float32)
    return hi, mid, rest - mid


def head_of(sp):
    z, y = sp // 4, sp % 4
    return (z // 2) * 2 + y // 2


def member_of(sp):
    z, y = sp // 4, sp % 4
    return (z % 2) * 2 + y % 2


def place_of(head, member):
    z = (head // 2) * 2 + member // 2
    y = (head % 2) * 2 + member % 2
    return z * 4 + y


def chunk_of(t, member):
    return (t // 2) * 8 + (member if t % 2 == 0 else 7 - member)


def ring():
    tp = lax.axis_index("tp")
    x, core = tp // 2, tp % 2
    right = ((x + 1) % 4) * 2 + core
    left = ((x + 3) % 4) * 2 + core
    far = ((x + 2) % 4) * 2 + core
    return tp, x * 2 + 1 - core, right, left, far


def greet_ring():
    tp, sibling, right, left, far = ring()
    barrier = pltpu.get_barrier_semaphore()
    for peer in (sibling, right, left):
        pl.semaphore_signal(barrier, inc=1, device_id={"tp": peer}, device_id_type=MESH)


class RingGather:
    def __init__(self, own, buf, send, recv):
        self.own, self.buf, self.send, self.recv = own, buf, send, recv
        self.rows = buf.shape[1]
        self.half = self.rows // 2
        self.count = 0

    def push(self, src, slot, peer, half=None):
        if half is None:
            dst, sem = self.buf.at[slot], self.recv.at[slot, 0]
        else:
            cut = pl.ds(half * self.half, self.half)
            dst, sem = self.buf.at[slot, cut], self.recv.at[slot, half]
        copy = pltpu.make_async_remote_copy(
            src_ref=src,
            dst_ref=dst,
            send_sem=self.send.at[self.count],
            recv_sem=sem,
            device_id={"tp": peer},
            device_id_type=MESH,
        )
        copy.start()
        self.count += 1

    def part(self, slot, half):
        return self.buf.at[slot, pl.ds(half * self.half, self.half)]

    def arrive(self, slot, half=None):
        if half is None:
            ref, sem = self.buf.at[slot], self.recv.at[slot, 0]
        else:
            ref, sem = self.part(slot, half), self.recv.at[slot, half]
        pltpu.make_async_copy(ref, ref, sem).wait()

    def begin(self):
        tp, sibling, right, left, far = ring()
        self.count = 0
        self.push(self.own, tp, right)
        self.push(self.own, tp, left)
        self.push(self.own, tp, sibling)

    def stage(self, n):
        tp, sibling, right, left, far = ring()
        self.count = 3 + 2 * n
        if n == 0:
            self.arrive(left)
            self.push(self.part(left, 0), left, right, 0)
            self.push(self.buf.at[left], left, sibling)
        elif n == 1:
            self.arrive(right)
            self.push(self.part(right, 1), right, left, 1)
            self.push(self.buf.at[right], right, sibling)
        else:
            for half in range(2):
                self.arrive(far, half)
                self.push(self.part(far, half), far, sibling, half)

    def relay(self):
        for n in range(3):
            self.stage(n)

    def finish(self):
        tp, sibling, right, left, far = ring()
        x = tp // 2
        other = 1 - tp % 2
        self.arrive(sibling)
        self.arrive(((x + 3) % 4) * 2 + other)
        self.arrive(((x + 1) % 4) * 2 + other)
        for half in range(2):
            self.arrive(((x + 2) % 4) * 2 + other, half)

    def sent(self):
        for n in range(9):
            ref = self.own if n not in (3, 5, 7, 8) else self.part(0, 0)
            pltpu.make_async_copy(ref, ref, self.send.at[n]).wait()


def greet_lines():
    me = lax.axis_index("sp")
    tp = lax.axis_index("tp")
    barrier = pltpu.get_barrier_semaphore()
    for n in range(1, 16):
        to = (me + n) % 16
        pl.semaphore_signal(barrier, inc=1, device_id={"sp": to}, device_id_type=MESH)
    for n in range(1, 8):
        to = (tp + n) % 8
        pl.semaphore_signal(barrier, inc=1, device_id={"tp": to}, device_id_type=MESH)


class GridGather:
    def __init__(self, buf, send, recv):
        self.buf, self.send, self.recv = buf, send, recv

    def view(self, phase, part, k, half=None):
        me = lax.axis_index("sp")
        z, y = me // 4, me % 4
        tail = (part,) if half is None else (part, half)
        if phase == 0:
            return self.buf.at[(z, k) + tail] if part == 0 else self.buf.at[(k, y) + tail]
        every = pl.ds(0, 4)
        return self.buf.at[(k, every) + tail] if part == 0 else self.buf.at[(every, k) + tail]

    def ring(self, phase, part):
        me = lax.axis_index("sp")
        z, y = me // 4, me % 4
        along_y = phase == part
        at = y if along_y else z
        right, left = (at + 1) % 4, (at + 3) % 4
        if along_y:
            return at, right, left, z * 4 + right, z * 4 + left
        return at, right, left, right * 4 + y, left * 4 + y

    def copies(self, phase, part):
        at, right, left, to_right, to_left = self.ring(phase, part)

        def one(n, view, to):
            return pltpu.make_async_remote_copy(
                src_ref=view,
                dst_ref=view,
                send_sem=self.send.at[phase, part, n],
                recv_sem=self.recv.at[phase, part, n],
                device_id={"sp": to},
                device_id_type=MESH,
            )

        return (
            one(0, self.view(phase, part, at), to_right),
            one(1, self.view(phase, part, at), to_left),
            one(2, self.view(phase, part, left, 0), to_right),
            one(3, self.view(phase, part, right, 1), to_left),
        )

    def begin(self, phase):
        for part in range(2):
            copies = self.copies(phase, part)
            copies[0].start()
            copies[1].start()

    def relay(self, phase):
        for part in range(2):
            copies = self.copies(phase, part)
            copies[0].wait_recv()
            copies[2].start()
            copies[1].wait_recv()
            copies[3].start()

    def finish(self, phase):
        for part in range(2):
            copies = self.copies(phase, part)
            copies[2].wait_recv()
            copies[3].wait_recv()

    def sent(self):
        for phase in range(2):
            for part in range(2):
                for copy in self.copies(phase, part):
                    copy.wait_send()


def layer_kernel(
    q_hbm, k_hbm, v_hbm, g_ref, w_ref, stream, gate_w, up_w, down_w, gain1, bias1, gain2, bias2,
    out,
    q_ref, k_ref, v_ref, att, wall, kvl, qt, ksrc, qsrc, X, R, S0, S1, S2, S3, mx0, mx1, mx2, mx3, M, A, O,
    G, D, rows, lhs, res, hid, pb, sib, zz, rel, inn, E, gt,
    ks, kr, qs, qr, ws, wr, ld, gs, gr, Gs, Gr, Ds, Dr, ns, nr, ss, sr, hs, hr, er, line,
):
    me = lax.axis_index("sp")
    tp = lax.axis_index("tp")
    z, y = me // 4, me % 4
    greet_lines()
    loads = [
        pltpu.make_async_copy(src, dst, ld.at[n])
        for n, (src, dst) in enumerate(
            (
                (k_hbm, k_ref),
                (v_hbm, v_ref),
                (q_hbm, q_ref),
                (w_ref, wall.at[tp]),
                (gate_w, gt.at[0]),
                (up_w, gt.at[1]),
                (down_w.at[pl.ds(0, 176)], D.at[z, y, 0, 0]),
                (down_w.at[pl.ds(176, 176)], D.at[z, y, 0, 1]),
                (down_w.at[pl.ds(352, 176)], D.at[z, y, 1, 0]),
                (down_w.at[pl.ds(528, 176)], D.at[z, y, 1, 1]),
                (stream.at[pl.ds(pl.multiple_of(tp * 96, 96), 96)], res),
            )
        )
    ]
    for load in loads:
        load.start()
    for load in loads[:3]:
        load.wait()
    kt = k_ref[...].T
    vt = v_ref[...].T
    qtt = q_ref[...].T
    gates = g_ref[...]
    row = lax.broadcasted_iota(jnp.int32, (16, BL), 0)
    for h in range(4):
        g = gates[h : h + 1]
        first = jnp.broadcast_to(g[:, 0:1], (1, BL))
        lines = [jnp.ones((1, BL), jnp.float32)]
        lines += parts((first - g) * LOG2E) + parts(first * (-LOG2E))
        extra = jnp.zeros((16, BL), jnp.float32)
        for n, r in enumerate(lines):
            extra = jnp.where(row == n, r, extra)
        ksrc[h, 0:64] = kt[64 * h : 64 * h + 64]
        ksrc[h, 64:80] = extra.astype(jnp.bfloat16)
        ksrc[h, 80:144] = vt[64 * h : 64 * h + 64]
        for i in range(3):
            qsrc[3 * h + i] = qtt[64 * h : 64 * h + 64, 256 * i : 256 * i + 256]
    pl.semaphore_wait(pltpu.get_barrier_semaphore(), 22)
    for n in range(1, 16):
        to = (me + n) % 16
        pl.semaphore_signal(line, inc=1, device_id={"sp": to}, device_id_type=MESH)
    qsends = []
    for h in range(4):
        for i in range(3):
            n = 3 * h + i
            sub = 3 * me + i
            c, u = sub // 2, sub % 2
            r = c % 8
            high = r // 4
            member = r + high * (7 - 2 * r)
            slot = 2 * ((c // 8) * 2 + high) + u
            to = place_of(h, member)
            copy = pltpu.make_async_remote_copy(
                src_ref=qsrc.at[n],
                dst_ref=qt.at[slot],
                send_sem=qs.at[n],
                recv_sem=qr.at[slot],
                device_id={"sp": to},
                device_id_type=MESH,
            )
            local = pltpu.make_async_copy(qsrc.at[n], qt.at[slot], qr.at[slot])

            @pl.when(to != me)
            def _():
                copy.start()

            @pl.when(to == me)
            def _():
                local.start()

            qsends.append((to, copy))
    own = pltpu.make_async_copy(ksrc.at[head_of(me)], kvl.at[me], kr.at[me])
    own.start()
    par = (z + y) % 2

    def axes(cls):
        return y + cls * (z - y), z + cls * (y - z)

    def dev(cls, a, c):
        return a * (1 + 3 * cls) + c * (4 - 3 * cls)

    def half_head(cls, a, c):
        return a * (1 + cls) + c * (2 - cls)

    def mate(k):
        return k + 1 - 2 * (k % 2)

    def pass_on(n, src, dst, sem, to):
        return pltpu.make_async_remote_copy(
            src_ref=src,
            dst_ref=dst,
            send_sem=ks.at[n],
            recv_sem=sem,
            device_id={"sp": to},
            device_id_type=MESH,
        )

    a, c = axes(par)
    ap, cp = a // 2, c // 2
    mine = (kvl.at[me], kr.at[me])
    side = (E.at[par, a], er.at[par, a])
    for n, (head, (dst, sem), to) in enumerate(
        (
            (half_head(par, 1 - ap, 1 - cp), side, dev(par, 3 - a, c)),
            (half_head(par, ap, 1 - cp), side, dev(par, mate(a), c)),
            (half_head(par, 1 - ap, cp), mine, dev(par, 3 - a, c)),
            (half_head(par, ap, cp), mine, dev(par, mate(a), c)),
            (half_head(par, ap, 1 - cp), mine, dev(par, a, 3 - c)),
            (half_head(par, ap, cp), mine, dev(par, a, mate(c))),
        )
    ):
        pass_on(n, ksrc.at[head], dst, sem, to).start()

    def fan(n, cls, b, slot):
        a, c = axes(cls)
        pltpu.make_async_copy(E.at[cls, slot], E.at[cls, slot], er.at[cls, slot]).wait()
        pass_on(n, E.at[cls, slot], kvl.at[b], kr.at[b], dev(cls, a, 3 - c)).start()
        pass_on(n + 1, kvl.at[b], kvl.at[b], kr.at[b], dev(cls, a, mate(c))).start()

    X_, Y_ = par, 1 - par
    xa, xc = axes(X_)
    ya, yc = axes(Y_)
    blocks = (
        me,
        dev(Y_, mate(ya), yc),
        dev(Y_, 3 - ya, yc),
        dev(Y_, ya, 3 - yc),
        dev(Y_, ya, mate(yc)),
        dev(X_, (xa + 2) % 4, xc),
        dev(X_, mate(xa), 3 - xc),
        dev(X_, 3 - xa, 3 - xc),
        dev(X_, mate(xa), mate(xc)),
        dev(X_, 3 - xa, mate(xc)),
        dev(Y_, (ya + 2) % 4, 3 - yc),
        dev(Y_, (ya + 2) % 4, mate(yc)),
        dev(X_, xa, (xc + 2) % 4),
        dev(Y_, mate(ya), (yc + 2) % 4),
        dev(Y_, 3 - ya, (yc + 2) % 4),
        dev(X_, (xa + 2) % 4, (xc + 2) % 4),
    )

    def arrive(n):
        b = blocks[n]
        pltpu.make_async_copy(ksrc.at[0], kvl.at[b], kr.at[b]).wait()
        block = kvl.at[b]
        if n == 1:
            fan(6, Y_, b, mate(ya))
        if n == 2:
            slot = 3 - ya
            to = dev(Y_, mate(ya), yc)
            pass_on(8, block, block, kr.at[b], to).start()
            fan(9, Y_, b, slot)
            pass_on(11, E.at[Y_, slot], E.at[Y_, slot], er.at[Y_, slot], to).start()
        if n == 5:
            fan(12, X_, b, (xa + 2) % 4)
        if n in (3, 10):
            pass_on(14 + n // 10, block, block, kr.at[b], dev(Y_, ya, mate(yc))).start()
        if n in (6, 7):
            pass_on(10 + n, block, block, kr.at[b], dev(X_, xa, mate(xc))).start()

    for load in loads[3:]:
        load.wait()
    gather = RingGather(wall.at[tp], wall, ws, wr)
    for n in range(2):
        turned = gt[n].T
        for half in range(2):
            G[z, y, half, n] = turned[64 * half : 64 * half + 64]
    upper = GridGather(G, Gs, Gr)
    lower = GridGather(D, Ds, Dr)

    row = lax.broadcasted_iota(jnp.int32, (64, QW), 0)
    ones = jnp.where((row >= 1) & (row < 4), 1.0, 0.0).astype(jnp.bfloat16)
    for t in range(NT):
        for u in range(2):
            pltpu.make_async_copy(qsrc.at[0], qt.at[2 * t + u], qr.at[2 * t + u]).wait()
        q = jnp.concatenate([qt[2 * t], qt[2 * t + 1]], axis=1).astype(jnp.float32)
        q = q * (LOG2E / 8)
        hi = q.astype(jnp.bfloat16)
        R[t, 0:64] = hi
        R[t, 64:128] = ones
        R[t, 128:192] = (q - hi.astype(jnp.float32)).astype(jnp.bfloat16)
        R[t, 192:256] = jnp.zeros((64, QW), jnp.bfloat16)
        M[t] = jnp.full((8, QW), NEG, jnp.float32)
        A[t] = jnp.zeros((80, QW), jnp.float32)

    mm = member_of(me)
    S = (S0, S1, S2, S3)
    mx = (mx0, mx1, mx2, mx3)

    def qk(t, n):
        x = X[...]
        s = jnp.dot(
            jnp.concatenate([x, x], axis=1), R[t], preferred_element_type=jnp.float32
        )
        S[n][...] = s
        mx[n][...] = jnp.max(s.reshape(BL // 8, 8, QW), axis=0)

    def mask(b, t, n):
        c = chunk_of(t, mm)

        @pl.when(b * BL + BL > c * QW)
        def _():
            kp = b * BL + lax.broadcasted_iota(jnp.int32, (BL, QW), 0)
            qp = c * QW + lax.broadcasted_iota(jnp.int32, (BL, QW), 1)
            s = jnp.where(kp <= qp, S[n][...], NEG)
            S[n][...] = s
            mx[n][...] = jnp.max(s.reshape(BL // 8, 8, QW), axis=0)

    def pv(b, t, n, bs):
        m_old = M[t][0:1]
        m_new = jnp.maximum(m_old, jnp.max(mx[n][...], axis=0, keepdims=True) + bs)
        p = jnp.exp2(S[n][...] - (m_new - bs)).astype(jnp.bfloat16)
        o = jnp.dot(kvl[b, 64:144], p, preferred_element_type=jnp.float32)
        A[t] = A[t] * jnp.exp2(m_old - m_new) + o
        M[t] = jnp.broadcast_to(m_new, (8, QW))

    def block(i, _):
        b = blocks[TURNS[0]]
        for n in range(1, 16):
            b = jnp.where(i == n, blocks[TURNS[n]], b)

        X[...] = kvl[b, 0:128, :].T
        g = kvl[b, 64:80, 0:128].astype(jnp.float32)
        bs = jnp.tile(g[4:5] + g[5:6] + g[6:7], (1, QW // 128))

        def live(t):
            return chunk_of(t, mm) * QW + QW > b * BL

        def ready(t):
            for n in (t, t + 1):
                if n < NT:
                    qk(n, n % 4)

        def masks(t):
            for n in (t, t + 1):
                if n < NT:
                    mask(b, n, n % 4)

        for t in range(0, NT, 2):

            @pl.when(live(t) if t == 0 else live(t) & jnp.logical_not(live(t - 1)))
            def _():
                ready(t)
                masks(t)

            @pl.when(live(t))
            def _():
                ready(t + 2)
                pv(b, t, t % 4, bs)
                pv(b, t + 1, (t + 1) % 4, bs)
                masks(t + 2)

            @pl.when(live(t + 1) & jnp.logical_not(live(t)))
            def _():
                qk(t + 1, (t + 1) % 4)
                mask(b, t + 1, (t + 1) % 4)
                ready(t + 2)
                pv(b, t + 1, (t + 1) % 4, bs)
                masks(t + 2)

        for n, arrivals in AFTER:

            @pl.when(i == n)
            def _():
                for k in arrivals:
                    arrive(k)

        @pl.when(i == 1)
        def _():
            gather.begin()

        for stage in range(3):

            @pl.when(i == RELAY[stage])
            def _():
                gather.stage(stage)

        @pl.when(i == 5)
        def _():
            upper.begin(0)
            lower.begin(0)

        @pl.when(i == 8)
        def _():
            upper.relay(0)
            lower.relay(0)

        @pl.when(i == 10)
        def _():
            upper.finish(0)
            upper.begin(1)

        return 0

    arrive(0)
    lax.fori_loop(0, 16, block, 0)

    head = tp * 4 + head_of(me)

    def piece(t, u, w):
        sub = 2 * chunk_of(t, mm) + u
        n = 8 * (sub % 3) + w
        to_sp, to_tp, spot = sub // 3, n // 3, n % 3
        src = O.at[(2 * t + u) * 8 + w]
        dst = att.at[head, spot]
        copy = pltpu.make_async_remote_copy(
            src_ref=src,
            dst_ref=dst,
            send_sem=gs.at[(2 * t + u) * 8 + w],
            recv_sem=gr,
            device_id={"sp": to_sp, "tp": to_tp},
            device_id_type=MESH,
        )
        return (to_sp == me) & (to_tp == tp), copy, src, dst

    for t in range(NT):
        a = A[t]
        heads = (a[16:80] / a[0:1]).T.astype(jnp.bfloat16)
        for n in range(16):
            O[16 * t + n] = jnp.concatenate(
                [heads[32 * n : 32 * n + 16], heads[32 * n + 16 : 32 * n + 32]], axis=1
            )
    pl.semaphore_wait(line, 15)
    for t in range(NT):
        for u in range(2):

            def send(w, _):
                mine, copy, src, dst = piece(t, u, w)

                @pl.when(jnp.logical_not(mine))
                def _():
                    copy.start()

                @pl.when(mine)
                def _():
                    pltpu.make_async_copy(src, dst, gr).start()

                return 0

            lax.fori_loop(0, 8, send, 0)
    lower.finish(0)
    lower.begin(1)
    upper.relay(1)
    gather.finish()
    pltpu.make_async_copy(att, att, gr).wait()
    for h in range(32):
        for n in range(3):
            lhs[32 * n : 32 * n + 16, HD * h : HD * h + HD] = att[h, n, :, 0:64]
            lhs[32 * n + 16 : 32 * n + 32, HD * h : HD * h + HD] = att[h, n, :, 64:128]
    mixed = jnp.dot(
        lhs[...], wall[...].reshape(2048, 2048), preferred_element_type=jnp.float32
    )
    mixed = mixed.astype(jnp.bfloat16).astype(jnp.float32)
    p = ALPHA * res[...].astype(jnp.float32) + mixed
    rows[tp] = layer_norm(p, gain1[...], bias1[...]).astype(jnp.bfloat16)
    spread = RingGather(rows.at[tp], rows, ns, nr)
    spread.begin()

    x, core = tp // 2, tp % 2
    _, sibling, right, left, far = ring()

    def project(chip):
        r = rows[pl.ds(2 * chip, 2)].reshape(192, 2048)
        gate = jnp.dot(
            r, G[:, :, :, 0].reshape(2048, 704), preferred_element_type=jnp.float32
        )
        up = jnp.dot(
            r, G[:, :, :, 1].reshape(2048, 704), preferred_element_type=jnp.float32
        )
        hid[chip] = (gate / (1.0 + jnp.exp(-gate)) * up).astype(jnp.bfloat16)

    other = 1 - core
    spread.stage(0)
    spread.stage(1)
    upper.finish(1)
    lower.relay(1)
    spread.arrive(sibling)
    chips = ((x + 2) % 4, (x + 1) % 4, (x + 3) % 4, x)

    def early(n, _):
        chip = (x + n - n // 2 + n % 2 * (1 - n // 2) * 2) % 4
        project(chip)

        @pl.when(n == 0)
        def _():
            spread.stage(2)
            spread.arrive(chips[2] * 2 + other)
            spread.arrive(chips[1] * 2 + other)

        @pl.when(n == 2)
        def _():
            for half in range(2):
                spread.arrive(chips[0] * 2 + other, half)

        return 0

    lax.fori_loop(0, 4, early, 0)
    lower.finish(1)

    def to_sibling(n):
        return pltpu.make_async_remote_copy(
            src_ref=pb.at[n, other],
            dst_ref=sib.at[n],
            send_sem=ss.at[n],
            recv_sem=sr.at[n],
            device_id={"tp": sibling},
            device_id_type=MESH,
        )

    def hop(n, src, dst, peer):
        return pltpu.make_async_remote_copy(
            src_ref=src,
            dst_ref=dst,
            send_sem=hs.at[n],
            recv_sem=hr.at[n],
            device_id={"tp": peer},
            device_id_type=MESH,
        )

    hops = [
        hop(0, zz.at[0, pl.ds(0, 48)], rel.at[0], right),
        hop(1, zz.at[0, pl.ds(48, 48)], rel.at[1], left),
        hop(2, zz.at[1], inn.at[0], right),
        hop(3, zz.at[2], inn.at[1], left),
    ]

    def product(n):
        wd = jnp.concatenate(
            [D[k // 4, k % 4].reshape(704, 128) for k in range(16)], axis=1
        )
        s = jnp.dot(hid[chips[n]], wd, preferred_element_type=jnp.float32)
        s = s.astype(jnp.bfloat16)
        pb[n, 0] = s[:96]
        pb[n, 1] = s[96:]
        to_sibling(n).start()

    def pair(n):
        to_sibling(n).wait_recv()
        return pb[n, core].astype(jnp.float32) + sib[n].astype(jnp.float32)

    product(0)
    product(1)
    zz[0] = pair(0).astype(jnp.bfloat16)
    hops[0].start()
    hops[1].start()
    product(2)
    s = pair(1)
    hops[0].wait_recv()
    zz[1, 0:48] = (s[:48] + rel[0].astype(jnp.float32)).astype(jnp.bfloat16)
    zz[1, 48:96] = s[48:].astype(jnp.bfloat16)
    hops[2].start()
    product(3)
    s = pair(2)
    hops[1].wait_recv()
    zz[2, 0:48] = s[:48].astype(jnp.bfloat16)
    zz[2, 48:96] = (s[48:] + rel[1].astype(jnp.float32)).astype(jnp.bfloat16)
    hops[3].start()
    s = pair(3)
    hops[2].wait_recv()
    hops[3].wait_recv()
    s = s + inn[0].astype(jnp.float32) + inn[1].astype(jnp.float32)
    lowered = s.astype(jnp.bfloat16).astype(jnp.float32)
    normed = rows[tp].astype(jnp.float32)
    out[...] = layer_norm(ALPHA * normed + lowered, gain2[...], bias2[...]).astype(jnp.bfloat16)
    for n in range(4):
        to_sibling(n).wait_send()
        hops[n].wait_send()
    spread.sent()
    upper.sent()
    lower.sent()
    for t in range(NT):
        for u in range(2):

            def sent(w, _):
                mine, copy, src, dst = piece(t, u, w)

                @pl.when(jnp.logical_not(mine))
                def _():
                    copy.wait_send()

                return 0

            lax.fori_loop(0, 8, sent, 0)
    gather.sent()
    for n in range(18):
        pltpu.make_async_copy(ksrc.at[0], ksrc.at[0], ks.at[n]).wait()
    for to, copy in qsends:

        @pl.when(to != me)
        def _():
            copy.wait_send()


def layer(*args):
    bf = jnp.bfloat16
    dma = pltpu.SemaphoreType.DMA
    scratch = [
        pltpu.VMEM((BL, 256), bf),
        pltpu.VMEM((BL, 256), bf),
        pltpu.VMEM((BL, 256), bf),
        pltpu.VMEM((32, 3, 16, 128), bf),
        pltpu.VMEM((8, 256, 2048), bf),
        pltpu.VMEM((NB, KVR, BL), bf),
        pltpu.VMEM((2 * NT, HD, 256), bf),
        pltpu.VMEM((4, KVR, BL), bf),
        pltpu.VMEM((12, HD, 256), bf),
        pltpu.VMEM((BL, 128), bf),
        pltpu.VMEM((NT, 256, QW), bf),
        pltpu.VMEM((BL, QW), jnp.float32),
        pltpu.VMEM((BL, QW), jnp.float32),
        pltpu.VMEM((BL, QW), jnp.float32),
        pltpu.VMEM((BL, QW), jnp.float32),
        pltpu.VMEM((8, QW), jnp.float32),
        pltpu.VMEM((8, QW), jnp.float32),
        pltpu.VMEM((8, QW), jnp.float32),
        pltpu.VMEM((8, QW), jnp.float32),
        pltpu.VMEM((NT, 8, QW), jnp.float32),
        pltpu.VMEM((NT, 80, QW), jnp.float32),
        pltpu.VMEM((96, 16, 128), bf),
        pltpu.VMEM((4, 4, 2, 2, 64, 704), bf),
        pltpu.VMEM((4, 4, 2, 2, 176, 128), bf),
        pltpu.VMEM((8, 96, 2048), bf),
        pltpu.VMEM((96, 2048), bf),
        pltpu.VMEM((96, 2048), bf),
        pltpu.VMEM((4, 192, 704), bf),
        pltpu.VMEM((4, 2, 96, 2048), bf),
        pltpu.VMEM((4, 96, 2048), bf),
        pltpu.VMEM((3, 96, 2048), bf),
        pltpu.VMEM((2, 48, 2048), bf),
        pltpu.VMEM((2, 96, 2048), bf),
        pltpu.VMEM((2, 4, KVR, BL), bf),
        pltpu.VMEM((2, 704, 128), bf),
        dma((18,)), dma((16,)), dma((12,)), dma((12,)), dma((9,)), dma((8, 2)), dma((13,)),
        dma((96,)), dma, dma((2, 2, 4)), dma((2, 2, 4)), dma((2, 2, 4)), dma((2, 2, 4)),
        dma((9,)), dma((8, 2)), dma((4,)), dma((4,)), dma((4,)), dma((4,)), dma((2, 4)),
        pltpu.SemaphoreType.REGULAR,
    ]
    return pl.pallas_call(
        layer_kernel,
        name="layer",
        out_shape=jax.ShapeDtypeStruct((96, 2048), bf),
        in_specs=[ANY] * 3 + [VMEM] + [ANY] * 5 + [VMEM] * 4,
        out_specs=VMEM,
        scratch_shapes=scratch,
        compiler_params=pltpu.CompilerParams(
            collective_id=0, has_side_effects=True, vmem_limit_bytes=62 * 2**20
        ),
    )(*args)


def body(
    queries,
    key_rows,
    value_rows,
    log_forget,
    stream_in,
    out_weight,
    mix_gain,
    mix_bias,
    gate_weight,
    up_weight,
    down_weight,
    ffn_gain,
    ffn_bias,
):
    return layer(
        queries,
        key_rows,
        value_rows,
        log_forget.T,
        out_weight,
        stream_in,
        gate_weight.T,
        up_weight.T,
        down_weight,
        mix_gain[None],
        mix_bias[None],
        ffn_gain[None],
        ffn_bias[None],
    )


def solution(mesh):
    placed = (
        P("sp", "tp"),
        P("sp", "tp"),
        P("sp", "tp"),
        P("sp", "tp"),
        P("sp", None),
        P("tp", None),
        P(),
        P(),
        P("sp", "tp"),
        P("sp", "tp"),
        P("tp", "sp"),
        P(),
        P(),
    )
    return jax.shard_map(
        body, mesh=mesh, in_specs=placed, out_specs=P(("sp", "tp"), None), check_vma=False
    )
```
